32 devices in a mesh: sp: 4 (over y, x), tp: 8 (over z, core).
Axes of the slice: x: 2, y: 2, z: 4, core: 2. Of those that a mesh axis runs over, the one named last changes fastest.
Arguments:
- lru_input: bfloat16 [1024, 2048], P('sp', 'tp'), may hold values from -27 to 27
- gate_input: bfloat16 [1024, 2048], P('sp', 'tp'), may hold values from -6 to 6
- documents: int32 [1024], P('sp'), may hold values from 0 to 1, never falling along the last dimension, each value on 1 to 768 neighbouring positions
- conv_taps: bfloat16 [4, 2048], P(None, 'tp'), may hold values from -3 to 3
- rate_weight: bfloat16 [16, 128, 128], P('tp'), may hold values from -0.5 to 0.5
- inlet_weight: bfloat16 [16, 128, 128], P('tp'), may hold values from -0.5 to 0.5
- decay_param: float32 [2048], P('tp')
- lru_gain: float32 [2048], P('tp'), may hold values from 0.1 to 1.9
- out_weight: bfloat16 [2048, 2048], P('tp'), may hold values from -0.125 to 0.125
- residual: bfloat16 [1024, 2048], P('sp'), may hold values from -6 to 6
- ffn_gain: float32 [2048], replicated, may hold values from 0.1 to 1.9
- routes: int32 [1024, 2], P('sp'), may hold values from 0 to 3, all different within a row; in each aligned block of 32 rows (0 to 31, 32 to 63, ...) at most 32 rows name the same one
- route_weights: float32 [1024, 2], P('sp'), may hold values from 0.1 to 0.9
- w_gate: bfloat16 [4, 2048, 6144], P('sp', None, 'tp'), may hold values from -0.125 to 0.125
- w_up: bfloat16 [4, 2048, 6144], P('sp', None, 'tp'), may hold values from -0.125 to 0.125
- w_down: bfloat16 [4, 6144, 2048], P('sp', 'tp'), may hold values from -0.078125 to 0.078125
Outputs:
- mixed_out: bfloat16 [1024, 2048], P(('sp', 'tp'))
The draws below stay inside these ranges and needn't reach their ends.
Inputs may be any that keep to these rules, and one draw needn't show every extreme that they name: `documents`: document numbers start at 0 and never fall along the sequence; a document spans at most 768 positions. `routes`: each row names 2 different experts. In each aligned block of 32 rows no expert is named by more than 32 rows, a bound that some block reaches.
All inputs are finite; a program needn't handle non-finite values.
Results may differ from the reference program's by a relative error of at most 0.017.
Values may be sent and summed in bfloat16 or wider, within the bound.
A program may use at most 64 MiB of HBM per device.

```python
import math
import jax
import jax.numpy as jnp
import numpy as np
from jax import lax

D = 2048
D_RNN = 2048
LRU_BLOCKS = 16
LRU_BLOCK = 128
CONV_TAPS = 4
FF = 6144
TOP = 2
TOKENS = 1024
ROUTE_ROWS = 32
EXPERTS = 4
CAP = 32
DOCS = 2
DOC_MOST = 768
N_TP = 8


def draw_lru_input(key, part):
    base_key, group_key, span_key = jax.random.split(jax.random.fold_in(key, 11), 3)
    group_levels = jax.random.uniform(group_key, (LRU_BLOCKS,), jnp.float32, -1.2, 1.2)
    span_levels = jax.random.uniform(span_key, (TOKENS // 64,), jnp.float32, -0.7, 0.7)
    channel_scale = jnp.repeat(jnp.exp(group_levels), LRU_BLOCK)
    position_scale = jnp.repeat(jnp.exp(span_levels), 64)
    base_values = jnp.clip(jax.random.normal(base_key, (TOKENS, D_RNN), jnp.float32), -4.0, 4.0)
    return (base_values * channel_scale[None, :] * position_scale[:, None]).astype(jnp.bfloat16)


def draw_decay_param(key, part):
    pick_key, slow_key, fast_key = jax.random.split(jax.random.fold_in(key, 23), 3)
    slow_share = 0.5
    slow_pick = jax.random.uniform(pick_key, (D_RNN,), jnp.float32) < slow_share
    slow_value = math.log(2.5 * TOKENS) + jax.random.uniform(slow_key, (D_RNN,), jnp.float32, 0.0, 1.5)
    fast_value = jnp.log(jax.random.uniform(fast_key, (D_RNN,), jnp.float32, 120.0, 400.0))
    return jnp.where(slow_pick, slow_value, fast_value).astype(jnp.float32)


def block_levels(rng, extent, pieces, smallest, largest):
    level = 1.0
    for axis_at, parts in pieces:
        steps = jax.random.uniform(jax.random.fold_in(jax.random.fold_in(rng, 6), axis_at), (parts,), jnp.float32, smallest / len(pieces), largest / len(pieces))
        level = level * jnp.repeat(jnp.exp(steps), extent[axis_at] // parts).reshape((-1,) + (1,) * (len(extent) - 1 - axis_at))
    return level


def profile(number_of, total, reach, slope):
    weights = [(1 << 20) // math.isqrt(standing ** slope) + 1 for standing in range(2, number_of + 1)]
    surplus, counts = total - reach - (number_of - 1), [1] * (number_of - 1)
    while surplus > 0:
        movable = [i for i in range(number_of - 1) if counts[i] < reach]
        pool, budget = sum([weights[i] for i in movable]), surplus
        for i in movable:
            more = min(reach - counts[i], max(1, budget * weights[i] // pool), surplus)
            counts[i] = counts[i] + more
            surplus = surplus - more
    return np.array([reach] + counts)


def ragged_sizes(key, count, total, bound, lean):
    if count == 2:
        one = jax.random.randint(key, (), max(1, total - bound), min(bound, total - 1) + 1)
        return jnp.stack([one, total - one])
    lengths = jnp.asarray(profile(count, total, bound, lean), jnp.int32)
    twos = (count - 1) // 2
    donor, receiver = lengths[1:1 + 2 * twos:2], lengths[2:2 + 2 * twos:2]
    slack = jnp.minimum(donor - 1, bound - receiver)
    moved = jax.random.randint(jax.random.fold_in(key, 1), (twos,), 0, 1 << 20) % (slack + 1)
    lengths = lengths.at[1:1 + 2 * twos:2].set(donor - moved).at[2:2 + 2 * twos:2].set(receiver + moved)
    return lengths[jax.random.permutation(jax.random.fold_in(key, 2), count)]


def deal_out(key, own, number, rows, number_of, top, limit, lean):
    sequence = jax.random.permutation(key, number_of)
    packed, common = load_shares(number_of, rows * top, limit, lean, True), load_shares(number_of, rows * top, limit, lean, False)
    places = jnp.arange(number_of)

    def named(tallies, rotation):
        used = int((tallies > 0).sum())
        fixed = max(1, used // 4)
        passed = fixed + (places - fixed + rotation * (used - fixed)) % max(1, number_of - fixed)
        return jnp.zeros((number_of,), jnp.int32).at[sequence[jnp.where(places < fixed, places, passed)]].set(jnp.asarray(tallies, jnp.int32))

    tallies = jnp.where(number % 4 == 0, named(packed, number // 4), named(common, number - number // 4 - 1))
    mixed = jax.random.permutation(jax.random.fold_in(own, 3), number_of)
    donor, sink = mixed[0:number_of // 2 * 2:2], mixed[1:number_of // 2 * 2:2]
    room = jnp.minimum(tallies[donor] - 1, limit - tallies[sink]) // 2
    room = jnp.where((donor == sequence[0]) | (sink == sequence[0]) | (tallies[sink] == 0), 0, jnp.maximum(room, 0))
    passed = jax.random.randint(jax.random.fold_in(own, 4), (number_of // 2,), 0, 1 << 20) % (room + 1)
    tallies = tallies.at[donor].add(-passed).at[sink].add(passed)
    members = jnp.searchsorted(jnp.cumsum(tallies), jnp.arange(rows * top), side="right").astype(jnp.int32)
    listing = members.reshape(top, rows).T
    listing = listing[jax.random.permutation(jax.random.fold_in(own, 1), rows)]
    rotation = jax.random.randint(jax.random.fold_in(own, 2), (rows, 1), 0, top)
    return jnp.take_along_axis(listing, (jnp.arange(top)[None, :] + rotation) % top, axis=1)


def load_shares(number_of, total, reach, slope, full):
    weights = [(1 << 20) // math.isqrt(grade ** slope) + 1 for grade in range(1, number_of + 1)]
    largest = reach if full else min(reach, max(-(-total // number_of), total * weights[0] // sum(weights)))
    least = 1 if total - largest >= number_of - 1 else 0
    given, rest = [largest] + [least] * (number_of - 1), total - largest - least * (number_of - 1)
    while rest > 0:
        movable = [i for i in range(1, number_of) if given[i] < largest] or [i for i in range(1, number_of) if given[i] < reach]
        whole, left = sum([weights[i] for i in movable]), rest
        for i in movable:
            more = min(reach - given[i], max(1, left * weights[i] // whole), rest)
            given[i] = given[i] + more
            rest = rest - more
    return np.array(given)


def normal_values(stream_key, dims, deviation, limit, cuts=(), kind=jnp.bfloat16):
    values = deviation * jax.random.normal(stream_key, dims, jnp.float32)
    if cuts:
        values = values * block_levels(stream_key, dims, cuts, -0.22, 0.18)
    return jnp.clip(values, -limit, limit).astype(kind)


def setup_inputs(seed: int = 0) -> dict:
    arg_keys = jax.random.split(jax.random.key(seed), 17)
    lru_input = draw_lru_input(jax.random.fold_in(arg_keys[16], 71), 0)
    gate_input = normal_values(arg_keys[1], (TOKENS, D_RNN), 1.0, 6.0, ((0, 4), (1, 8)))
    documents = jnp.searchsorted(jnp.cumsum(ragged_sizes(arg_keys[2], DOCS, TOKENS, DOC_MOST, 0)), jnp.arange(TOKENS), side="right").astype(jnp.int32)
    conv_taps = normal_values(arg_keys[3], (CONV_TAPS, D_RNN), CONV_TAPS ** -0.5, 3.0, ((1, 8),))
    rate_weight = normal_values(arg_keys[4], (LRU_BLOCKS, LRU_BLOCK, LRU_BLOCK), LRU_BLOCK ** -0.5, 0.5, ((0, 8),))
    inlet_weight = normal_values(arg_keys[5], (LRU_BLOCKS, LRU_BLOCK, LRU_BLOCK), LRU_BLOCK ** -0.5, 0.5, ((0, 8),))
    decay_param = draw_decay_param(jax.random.fold_in(arg_keys[16], 71), 0)
    lru_gain = jnp.clip(1.0 + 0.18 * jax.random.normal(arg_keys[7], (D_RNN,), jnp.float32), 0.1, 1.9)
    out_weight = normal_values(arg_keys[8], (D_RNN, D), D_RNN ** -0.5, 0.125, ((0, 8),))
    residual = normal_values(arg_keys[9], (TOKENS, D), 1.0, 6.0, ((0, 4),))
    ffn_gain = jnp.clip(1.0 + 0.18 * jax.random.normal(arg_keys[10], (D,), jnp.float32), 0.1, 1.9)
    routes_keys = jax.random.split(jax.random.fold_in(arg_keys[11], 1), TOKENS // ROUTE_ROWS)
    routes_turns = jax.random.permutation(jax.random.fold_in(arg_keys[11], 3), TOKENS // ROUTE_ROWS)
    routes = jax.vmap(lambda own, number: deal_out(jax.random.fold_in(arg_keys[11], 2), own, number, ROUTE_ROWS, EXPERTS, TOP, CAP, 2))(routes_keys, routes_turns).reshape((TOKENS, TOP))
    route_weights = jnp.clip(0.1 + 0.79999997 * jax.random.uniform(arg_keys[12], (TOKENS, TOP), jnp.float32) ** block_levels(arg_keys[12], (TOKENS, TOP), ((0, 4),), -0.2, 0.2), 0.1, 0.9)
    w_gate = normal_values(arg_keys[13], (EXPERTS, D, FF), D ** -0.5, 0.125, ((0, 4), (2, 8)))
    w_up = normal_values(arg_keys[14], (EXPERTS, D, FF), D ** -0.5, 0.125, ((0, 4), (2, 8)))
    w_down = normal_values(arg_keys[15], (EXPERTS, FF, D), FF ** -0.5, 0.078125, ((0, 4), (1, 8)))
    return {"lru_input": lru_input, "gate_input": gate_input, "documents": documents, "conv_taps": conv_taps, "rate_weight": rate_weight, "inlet_weight": inlet_weight, "decay_param": decay_param, "lru_gain": lru_gain, "out_weight": out_weight, "residual": residual, "ffn_gain": ffn_gain, "routes": routes, "route_weights": route_weights, "w_gate": w_gate, "w_up": w_up, "w_down": w_down}


EPSILON = 1e-06
RATE_SCALE = 8.0

def join_runs(earlier_run, later_run):
    return (earlier_run[0] * later_run[0], later_run[0] * earlier_run[1] + later_run[1])

def slot_targets(route_block, expert_count, capacity):
    flat_routes = route_block.reshape(-1)
    onehot = (flat_routes[:, None] == jnp.arange(expert_count, dtype=jnp.int32)[None, :]).astype(jnp.int32)
    earlier_hits = jnp.cumsum(onehot, axis=0) - onehot
    slot_index = lax.optimization_barrier(jnp.sum(earlier_hits * onehot, axis=1))
    return (flat_routes * capacity + slot_index).astype(jnp.int32).reshape(route_block.shape)

def rms_rows(row_block, gain_vector):
    floated = row_block.astype(jnp.float32)
    inverse_rms = lax.rsqrt(lax.optimization_barrier(jnp.mean(floated * floated, axis=1, keepdims=True)) + EPSILON)
    return (floated * inverse_rms * gain_vector.astype(jnp.float32)[None, :]).astype(jnp.bfloat16)

def summed_blocks(left_rows, right_rows, blocks):
    span_width = left_rows.shape[1] // blocks

    def add_block(running, block_index):
        start_col = (block_index * span_width).astype(jnp.int32)
        partial_sum = jnp.dot(lax.dynamic_slice_in_dim(left_rows, start_col, span_width, 1), lax.dynamic_slice_in_dim(right_rows, start_col, span_width, 0), preferred_element_type=jnp.float32)
        partial_sum = lax.optimization_barrier(partial_sum.astype(jnp.bfloat16)).astype(jnp.float32)
        return (running + partial_sum, None)
    running, _ = lax.scan(add_block, jnp.zeros((left_rows.shape[0], right_rows.shape[1]), jnp.float32), jnp.arange(blocks, dtype=jnp.int32))
    return running

def reference(lru_input, gate_input, documents, conv_taps, rate_weight, inlet_weight, decay_param, lru_gain, out_weight, residual, ffn_gain, routes, route_weights, w_gate, w_up, w_down):
    documents = documents.astype(jnp.int32)
    reach_back = CONV_TAPS - 1
    prior_docs = jnp.concatenate([jnp.full((reach_back,), -1, jnp.int32), documents])
    padded_input = jnp.concatenate([jnp.zeros((reach_back, D_RNN), jnp.bfloat16), lru_input], axis=0)
    conv_sum = jnp.zeros((TOKENS, D_RNN), jnp.float32)
    for tap_index in range(CONV_TAPS):
        same_doc = (prior_docs[tap_index:tap_index + TOKENS] == documents).astype(jnp.float32)[:, None]
        conv_sum = conv_sum + padded_input[tap_index:tap_index + TOKENS].astype(jnp.float32) * conv_taps[tap_index].astype(jnp.float32)[None, :] * same_doc
    convolved = conv_sum.astype(jnp.bfloat16)
    grouped = convolved.astype(jnp.float32).reshape(TOKENS, LRU_BLOCKS, LRU_BLOCK)
    rate_gate = jax.nn.sigmoid(jnp.einsum('tnc,ncd->tnd', grouped, rate_weight.astype(jnp.float32)).reshape(TOKENS, D_RNN))
    inlet_gate = jax.nn.sigmoid(jnp.einsum('tnc,ncd->tnd', grouped, inlet_weight.astype(jnp.float32)).reshape(TOKENS, D_RNN))
    log_decay = -RATE_SCALE * rate_gate * jax.nn.softplus(-decay_param.astype(jnp.float32))[None, :]
    starts = (prior_docs[reach_back - 1:reach_back - 1 + TOKENS] != documents)[:, None]
    decay_step = jnp.where(starts, 0.0, jnp.exp(log_decay))
    norm_factor = jnp.where(starts, 1.0, jnp.sqrt(-jnp.expm1(2.0 * log_decay)))
    drive_term = norm_factor * inlet_gate * convolved.astype(jnp.float32)
    _, hidden_state = lax.associative_scan(join_runs, (decay_step, drive_term), axis=0)
    inverse_rms = lax.rsqrt(lax.optimization_barrier(jnp.mean(hidden_state * hidden_state, axis=1, keepdims=True)) + EPSILON)
    mixer_rows = (hidden_state * inverse_rms * lru_gain.astype(jnp.float32)[None, :] * jax.nn.gelu(gate_input.astype(jnp.float32))).astype(jnp.bfloat16)
    projected = summed_blocks(mixer_rows, out_weight, N_TP)
    after_mixer = (residual.astype(jnp.float32) + projected).astype(jnp.bfloat16)
    normed = rms_rows(after_mixer, ffn_gain)
    block_count = TOKENS // ROUTE_ROWS
    route_blocks = routes.astype(jnp.int32).reshape(block_count, ROUTE_ROWS, TOP)

    def block_slots(route_block):
        return slot_targets(route_block, EXPERTS, CAP)
    targets = jax.vmap(block_slots)(route_blocks)
    slot_index = targets - route_blocks * CAP
    block_ids = jnp.arange(block_count, dtype=jnp.int32)[:, None, None]
    buffer_rows = ((route_blocks * block_count + block_ids) * CAP + slot_index).astype(jnp.int32).reshape(-1)
    token_ids = jnp.broadcast_to(jnp.arange(TOKENS, dtype=jnp.int32).reshape(block_count, ROUTE_ROWS, 1), route_blocks.shape).reshape(-1)
    slot_table = jnp.zeros((EXPERTS * block_count * CAP,), jnp.int32).at[buffer_rows].set(token_ids + 1)
    padded_normed = jnp.concatenate([jnp.zeros((1, D), jnp.bfloat16), normed], axis=0)
    expert_span = block_count * CAP

    def run_expert(expert_id):
        picked_ids = lax.dynamic_slice_in_dim(slot_table, (expert_id * expert_span).astype(jnp.int32), expert_span, 0)
        expert_in = padded_normed[picked_ids]
        gate_part = jnp.dot(expert_in, w_gate[expert_id], preferred_element_type=jnp.float32)
        up_part = jnp.dot(expert_in, w_up[expert_id], preferred_element_type=jnp.float32)
        hidden_units = (jax.nn.silu(gate_part) * up_part).astype(jnp.bfloat16)
        return summed_blocks(hidden_units, w_down[expert_id], N_TP).astype(jnp.bfloat16)
    expert_out = lax.map(run_expert, jnp.arange(EXPERTS, dtype=jnp.int32))
    gathered = expert_out.reshape(EXPERTS * expert_span, D)[buffer_rows].astype(jnp.float32).reshape(TOKENS, TOP, D)
    routed = lax.optimization_barrier(jnp.sum(gathered * route_weights.astype(jnp.float32)[:, :, None], axis=1))
    return (after_mixer.astype(jnp.float32) + routed).astype(jnp.bfloat16)
```

```python
import functools

import jax
import jax.numpy as jnp
from jax import lax
from jax.experimental import pallas as pl
from jax.experimental.pallas import tpu as pltpu
from jax.sharding import PartitionSpec as P

D_RNN = 2048


EPSILON = 1e-06
RATE_SCALE = 8.0


def shifted(block, axis, distance):
    devices = range(lax.axis_size(axis))
    route = [(i - distance, i) for i in devices if i - distance in devices]
    return lax.ppermute(block, axis, route)


def carried_in(value, axis, join, neutral):
    count, mine = (lax.axis_size(axis), lax.axis_index(axis))
    pieces = jax.tree.map(lambda part: lax.all_gather(part, axis), value)
    so_far = jax.tree.map(
        lambda part, zero: jnp.full_like(part, 0) + jnp.asarray(zero, part.dtype), value, neutral
    )

    def hop(position, so_far):
        longer = join(so_far, jax.tree.map(lambda part: part[position], pieces))
        return jax.tree.map(lambda new, old: jnp.where(position < mine, new, old), longer, so_far)

    return lax.fori_loop(0, count - 1, hop, so_far)


def join_runs(earlier_run, later_run):
    return (earlier_run[0] * later_run[0], later_run[0] * earlier_run[1] + later_run[1])


def slot_targets(route_block, expert_count, capacity):
    flat_routes = route_block.reshape(-1)
    onehot = (flat_routes[:, None] == jnp.arange(expert_count, dtype=jnp.int32)[None, :]).astype(
        jnp.int32
    )
    earlier_hits = jnp.cumsum(onehot, axis=0) - onehot
    slot_index = jnp.sum(earlier_hits * onehot, axis=1)
    return (flat_routes * capacity + slot_index).reshape(route_block.shape)


def pick_matrix(targets, slot_total):
    slot_hits = targets[None, :, :] == jnp.arange(slot_total, dtype=jnp.int32)[:, None, None]
    return jnp.sum(slot_hits.astype(jnp.int32), axis=2).astype(jnp.bfloat16)


def rms_rows(row_block, gain_vector):
    floated = row_block.astype(jnp.float32)
    inverse_rms = lax.rsqrt(jnp.mean(floated * floated, axis=1, keepdims=True) + EPSILON)
    return (floated * inverse_rms * gain_vector[None, :]).astype(jnp.bfloat16)


def expert_apply(row_piece, gate_weight, up_weight, down_weight):
    gate_part = jnp.dot(row_piece, gate_weight, preferred_element_type=jnp.float32)
    up_part = jnp.dot(row_piece, up_weight, preferred_element_type=jnp.float32)
    hidden_units = (jax.nn.silu(gate_part) * up_part).astype(jnp.bfloat16)
    return jnp.dot(hidden_units, down_weight, preferred_element_type=jnp.float32)


def local(
    lru_input,
    gate_input,
    documents,
    conv_taps,
    rate_weight,
    inlet_weight,
    decay_param,
    lru_gain,
    out_weight,
    residual,
    ffn_gain,
    routes,
    route_weights,
    w_gate,
    w_up,
    w_down,
):
    positions = lru_input.shape[0]
    channels = lru_input.shape[1]
    model_width = residual.shape[1]
    reach_back = conv_taps.shape[0] - 1
    tail_rows, tail_docs = shifted(
        (lru_input[positions - reach_back :], documents[positions - reach_back :] + 1), "sp", 1
    )
    prior_docs = jnp.concatenate([tail_docs - 1, documents])
    padded_input = jnp.concatenate([tail_rows, lru_input], axis=0)
    conv_sum = jnp.zeros((positions, channels), jnp.float32)
    for tap_index in range(reach_back + 1):
        same_doc = (prior_docs[tap_index : tap_index + positions] == documents).astype(jnp.float32)[
            :, None
        ]
        conv_sum = (
            conv_sum
            + padded_input[tap_index : tap_index + positions].astype(jnp.float32)
            * conv_taps[tap_index].astype(jnp.float32)[None, :]
            * same_doc
        )
    convolved = conv_sum.astype(jnp.bfloat16)
    grouped = convolved.reshape(positions, rate_weight.shape[0], rate_weight.shape[1])
    rate_gate = jax.nn.sigmoid(
        jnp.einsum(
            "tnc,ncd->tnd", grouped, rate_weight, preferred_element_type=jnp.float32
        ).reshape(positions, channels)
    )
    inlet_gate = jax.nn.sigmoid(
        jnp.einsum(
            "tnc,ncd->tnd", grouped, inlet_weight, preferred_element_type=jnp.float32
        ).reshape(positions, channels)
    )
    log_decay = -RATE_SCALE * rate_gate * jax.nn.softplus(-decay_param)[None, :]
    starts = (prior_docs[reach_back - 1 : reach_back - 1 + positions] != documents)[:, None]
    decay_step = jnp.where(starts, 0.0, jnp.exp(log_decay))
    norm_factor = jnp.where(starts, 1.0, jnp.sqrt(-jnp.expm1(2.0 * log_decay)))
    drive_term = norm_factor * inlet_gate * convolved.astype(jnp.float32)
    decay_run, local_state = lax.associative_scan(join_runs, (decay_step, drive_term), axis=0)
    carried = carried_in(
        (decay_run[positions - 1], local_state[positions - 1]),
        "sp",
        join_runs,
        (jnp.ones((channels,), jnp.float32), jnp.zeros((channels,), jnp.float32)),
    )
    hidden_state = local_state + decay_run * carried[1][None, :]
    square_sums = lax.psum(jnp.sum(hidden_state * hidden_state, axis=1), "tp")
    inverse_rms = lax.rsqrt(square_sums[:, None] / D_RNN + EPSILON)
    mixer_rows = (
        hidden_state * inverse_rms * lru_gain[None, :] * jax.nn.gelu(gate_input.astype(jnp.float32))
    ).astype(jnp.bfloat16)
    tp_count = lax.axis_size("tp")
    tp_here = lax.axis_index("tp")
    expert_count = lax.axis_size("sp")
    route_rows = positions // tp_count
    top_count = routes.shape[1]
    capacity = 2 * top_count * route_rows // expert_count
    slot_total = expert_count * capacity
    projected = lax.psum_scatter(
        jnp.dot(mixer_rows, out_weight, preferred_element_type=jnp.float32).astype(jnp.bfloat16),
        "tp",
        scatter_dimension=0,
        tiled=True,
    ).astype(jnp.float32)
    own_rows = (
        lax.dynamic_slice_in_dim(residual, tp_here * route_rows, route_rows, 0).astype(jnp.float32)
        + projected
    ).astype(jnp.bfloat16)
    own_routes = lax.dynamic_slice_in_dim(routes, tp_here * route_rows, route_rows, 0)
    targets = slot_targets(own_routes, expert_count, capacity)
    outgoing = jnp.dot(
        pick_matrix(targets, slot_total),
        rms_rows(own_rows, ffn_gain),
        preferred_element_type=jnp.float32,
    ).astype(jnp.bfloat16)
    arrived = lax.all_to_all(
        outgoing.reshape(expert_count, capacity, model_width),
        "sp",
        split_axis=0,
        concat_axis=0,
        tiled=True,
    )
    partial_out = expert_apply(
        lax.all_gather(arrived.reshape(slot_total, model_width), "tp", axis=0, tiled=True),
        w_gate[0],
        w_up[0],
        w_down[0],
    )
    expert_out = lax.psum_scatter(
        partial_out.astype(jnp.bfloat16), "tp", scatter_dimension=0, tiled=True
    )
    returned = lax.all_to_all(
        expert_out.reshape(expert_count, capacity, model_width),
        "sp",
        split_axis=0,
        concat_axis=0,
        tiled=True,
    )
    picked = returned.reshape(slot_total, model_width)[targets.reshape(-1)].astype(jnp.float32)
    picked = picked.reshape(route_rows, top_count, model_width)
    own_weights = lax.dynamic_slice_in_dim(route_weights, tp_here * route_rows, route_rows, 0)
    routed = jnp.sum(picked * own_weights[:, :, None], axis=1)
    return (own_rows.astype(jnp.float32) + routed).astype(jnp.bfloat16)


MESH = pl.DeviceIdType.MESH
LANES = 128
GELU_SCALE = 0.7978845608028654


def sender(source, target, send_sem, recv_sem, peer):
    return pltpu.make_async_remote_copy(
        src_ref=source,
        dst_ref=target,
        send_sem=send_sem,
        recv_sem=recv_sem,
        device_id=peer,
        device_id_type=MESH,
    )


def greet(peers):
    barrier = pltpu.get_barrier_semaphore()
    for peer in peers:
        pl.semaphore_signal(barrier, inc=1, device_id=peer, device_id_type=MESH)
    pl.semaphore_wait(barrier, len(peers))


def one_minus_exp(value):
    series = 1.0 + value * (1.0 / 6.0)
    for order in (5.0, 4.0, 3.0, 2.0):
        series = 1.0 + value * (1.0 / order) * series
    return jnp.where(value > -0.25, -value * series, 1.0 - jnp.exp(value))


def down_by(block, distance, filler):
    count = block.shape[0]
    if distance % 8 == 0:
        top = jnp.full((distance, block.shape[1]), filler, block.dtype)
        return jnp.concatenate([top, block[: count - distance]], axis=0)
    row = lax.broadcasted_iota(jnp.int32, block.shape, 0)
    return jnp.where(row >= distance, pltpu.roll(block, distance, 0), filler)


def front_kernel(
    n_sp,
    n_tp,
    lru_ref,
    gate_ref,
    docs_ref,
    taps_ref,
    rate_ref,
    inlet_ref,
    decay_ref,
    gain_ref,
    out_w_ref,
    residual_ref,
    ffn_ref,
    weights_ref,
    own_ref,
    normed_ref,
    shares_ref,
    halo_x,
    halo_d,
    carry_out,
    carry_in,
    share_in,
    run_a,
    run_b,
    parts,
    pair_in,
    z_out,
    z_in,
    squares,
    square_pair,
    square_out,
    square_in,
    res_rows,
    res_sem,
    halo_s,
    halo_r,
    carry_s,
    carry_r,
    share_s,
    share_r,
    pair_s,
    pair_r,
    z_s,
    z_r,
):
    me_s, me_t = lax.axis_index("sp"), lax.axis_index("tp")
    n_z = n_tp // 2
    me_z, me_c = me_t // 2, me_t % 2
    rows, channels = lru_ref.shape
    width = out_w_ref.shape[1]
    piece = rows // n_tp
    residual_copy = pltpu.make_async_copy(
        residual_ref.at[pl.ds(pl.multiple_of(me_t * piece, piece), piece)], res_rows, res_sem
    )
    residual_copy.start()
    sp_peers = [((me_s + k) % n_sp, me_t) for k in range(1, n_sp)]
    tp_peers = [(me_s, (me_t + k) % n_tp) for k in range(1, n_tp)]
    greet(sp_peers + tp_peers)
    halo = [
        sender(lru_ref.at[pl.ds(rows - 16, 16)], halo_x, halo_s.at[0], halo_r.at[0], sp_peers[0]),
        sender(docs_ref.at[pl.ds(rows - 8, 8)], halo_d, halo_s.at[1], halo_r.at[1], sp_peers[0]),
    ]
    for copy in halo:
        copy.start()
    share = [
        sender(weights_ref, share_in.at[me_s], share_s.at[k], share_r.at[k], peer)
        for k, peer in enumerate(sp_peers)
    ]
    for copy in share:
        copy.start()
    for copy in halo:
        copy.wait()

    docs = docs_ref[...]
    before = jnp.where(me_s == 0, jnp.int32(-1), halo_d[...])
    docs_long = jnp.concatenate([before, docs], axis=0)
    taps = taps_ref[...].astype(jnp.float32)
    starts = docs_long[7 : 7 + rows] != docs
    for group in range(channels // LANES):
        span = slice(group * LANES, (group + 1) * LANES)
        long = jnp.concatenate(
            [halo_x[:, span].astype(jnp.float32)[8:], lru_ref[:, span].astype(jnp.float32)], axis=0
        )
        total = jnp.zeros((rows, LANES), jnp.float32)
        for tap in range(taps.shape[0]):
            first = 8 - (taps.shape[0] - 1) + tap
            same = docs_long[first : first + rows] == docs
            total = total + jnp.where(same, long[first : first + rows], 0.0) * taps[tap : tap + 1, span]
        convolved = total.astype(jnp.bfloat16)
        rate = jax.nn.sigmoid(
            jnp.dot(convolved, rate_ref[group], preferred_element_type=jnp.float32)
        )
        inlet = jax.nn.sigmoid(
            jnp.dot(convolved, inlet_ref[group], preferred_element_type=jnp.float32)
        )
        minus = -decay_ref[:, span]
        soft = jnp.maximum(minus, 0.0) + jnp.log1p(jnp.exp(-jnp.abs(minus)))
        log_decay = -RATE_SCALE * rate * soft
        step = jnp.where(starts, 0.0, jnp.exp(log_decay))
        factor = jnp.where(starts, 1.0, jnp.sqrt(one_minus_exp(2.0 * log_decay)))
        state = factor * inlet * convolved.astype(jnp.float32)
        distance = 1
        while distance < rows:
            state = state + step * down_by(state, distance, 0.0)
            step = step * down_by(step, distance, 1.0)
            distance *= 2
        run_a[:, span] = step
        run_b[:, span] = state
        carry_out[:, span] = jnp.concatenate(
            [step[rows - 1 :], state[rows - 1 :], jnp.zeros((6, LANES), jnp.float32)], axis=0
        )
    carry = [
        sender(carry_out, carry_in.at[me_s], carry_s.at[k], carry_r.at[k], peer)
        for k, peer in enumerate(sp_peers)
    ]
    for copy in carry:
        copy.start()
    carry_in[pl.ds(me_s, 1)] = carry_out[...][None]
    raw = gate_ref[...].astype(jnp.float32)
    gelu = 0.5 * raw * (1.0 + jnp.tanh(GELU_SCALE * (raw + 0.044715 * raw * raw * raw)))
    gelu = gelu * gain_ref[...]
    for copy in carry:
        copy.wait()
    carried = jnp.zeros((1, channels), jnp.float32)
    for place in range(n_sp - 1):
        tile = carry_in[place]
        carried = jnp.where(place < me_s, tile[1:2] + tile[0:1] * carried, carried)
    hidden = run_b[...] + run_a[...] * carried
    row_squares = jnp.sum(hidden * hidden, axis=1, keepdims=True)
    squares[...] = jnp.broadcast_to(row_squares, (rows, LANES)).reshape(n_tp, piece, LANES)
    mixer = (hidden * gelu).astype(jnp.bfloat16)
    tile_width = min(512, width)
    for first in range(0, width, tile_width):
        span = slice(first, first + tile_width)
        product = jnp.dot(mixer, out_w_ref[:, span], preferred_element_type=jnp.float32)
        parts[:, :, span] = product.astype(jnp.bfloat16).reshape(n_tp, piece, tile_width)

    partner = (me_s, me_z * 2 + 1 - me_c)
    order = [(me_z + k) % n_z for k in range(1, n_z + 1)]
    pair = []
    for i, z in enumerate(order):
        theirs = z * 2 + 1 - me_c
        pair.append(
            (
                sender(parts.at[theirs], pair_in.at[i], pair_s.at[0, i], pair_r.at[0, i], partner),
                sender(
                    squares.at[theirs], square_pair.at[i], pair_s.at[1, i], pair_r.at[1, i], partner
                ),
            )
        )
        for copy in pair[-1]:
            copy.start()
    z_copies = []
    for i, z in enumerate(order):
        mine = z * 2 + me_c
        for copy in pair[i]:
            copy.wait_recv()
        z_out[i] = (
            parts[mine].astype(jnp.float32) + pair_in[i].astype(jnp.float32)
        ).astype(jnp.bfloat16)
        square_out[i] = squares[mine] + square_pair[i]
        if i < n_z - 1:
            peer = (me_s, mine)
            copies = (
                sender(z_out.at[i], z_in.at[i], z_s.at[0, i], z_r.at[0, i], peer),
                sender(square_out.at[i], square_in.at[i], z_s.at[1, i], z_r.at[1, i], peer),
            )
            for copy in copies:
                copy.start()
            z_copies.append(copies)
    summed = z_out[n_z - 1].astype(jnp.float32)
    square_sum = square_out[n_z - 1]
    for i in range(n_z - 1):
        for copy in z_copies[i]:
            copy.wait_recv()
        summed = summed + z_in[i].astype(jnp.float32)
        square_sum = square_sum + square_in[i]
    inverse = lax.rsqrt(square_sum[:, :1] / (channels * n_tp) + EPSILON)
    residual_copy.wait()
    own = (res_rows[...].astype(jnp.float32) + summed * inverse).astype(jnp.bfloat16)
    own_ref[...] = own
    floated = own.astype(jnp.float32)
    inverse = lax.rsqrt(jnp.mean(floated * floated, axis=1, keepdims=True) + EPSILON)
    normed_ref[...] = (floated * inverse * ffn_ref[...]).astype(jnp.bfloat16)
    for copy in share:
        copy.wait()
    share_in[pl.ds(me_s, 1)] = weights_ref[...][None]
    shares_ref[...] = share_in[...]
    for copies in pair + z_copies:
        for copy in copies:
            copy.wait_send()


def expert_kernel(
    n_sp,
    n_tp,
    normed_ref,
    own_ref,
    shares_ref,
    gate_hbm,
    up_hbm,
    down_hbm,
    out_ref,
    w_gate,
    w_up,
    w_down,
    blocks,
    hidden,
    products,
    pair_in,
    joined,
    first_x,
    first_y,
    second_x,
    second_y,
    relay_a,
    relay_b,
    column,
    z_in,
    w_sem,
    own_sem,
    gz_s,
    gz_r,
    gxy_s,
    gxy_r,
    gd_s,
    gd_r,
    gp_s,
    gp_r,
    rp_s,
    rp_r,
    r1_s,
    r1_r,
    r2_s,
    r2_r,
    rz_s,
    rz_r,
):
    me_s, me_t = lax.axis_index("sp"), lax.axis_index("tp")
    n_z = n_tp // 2
    me_z, me_c = me_t // 2, me_t % 2
    piece, width = normed_ref.shape
    half = width // 2
    lower, upper = pl.ds(0, half), pl.ds(half, half)
    loads = [
        pltpu.make_async_copy(source, target, w_sem.at[k])
        for k, (source, target) in enumerate(
            ((gate_hbm, w_gate), (up_hbm, w_up), (down_hbm, w_down))
        )
    ]
    for copy in loads:
        copy.start()
    own_copy = pltpu.make_async_copy(normed_ref, blocks.at[me_s, me_t], own_sem)
    own_copy.start()
    s_x = me_s + 1 - 2 * (me_s % 2)
    s_y = (me_s + 2) % n_sp
    s_d = n_sp - 1 - me_s
    groups = (me_s, s_x, s_y, s_d)
    x_peer, y_peer = (s_x, me_t), (s_y, me_t)
    partner = (me_s, me_z * 2 + 1 - me_c)
    z_peers = [(me_s, ((me_z + k) % n_z) * 2 + me_c) for k in range(1, n_z)]
    greet([x_peer, y_peer, partner] + z_peers)

    sent = []

    def push(source, target, sems, slot, peer):
        copy = sender(source, target, sems[0].at[slot], sems[1].at[slot], peer)
        copy.start()
        sent.append(copy)
        return copy

    gz, gxy, gd, gp = (gz_s, gz_r), (gxy_s, gxy_r), (gd_s, gd_r), (gp_s, gp_r)
    arrive = [((me_z + n_z - i) % n_z) * 2 + me_c for i in range(n_z)]
    mine = blocks.at[me_s, me_t]
    from_x, from_y, from_da, from_db, from_z = {}, {}, {}, {}, {}
    from_pair = {}
    for k in range(n_z - 1):
        from_z[k + 1] = push(normed_ref, mine, gz, k, z_peers[k])
    from_x[0] = push(normed_ref, mine, gxy, (0, 0), x_peer)
    from_y[0] = push(normed_ref, mine, gxy, (1, 0), y_peer)
    from_pair[0, 0] = push(normed_ref, mine, gp, (0, 0), partner)

    def relay_xy(i):
        t = arrive[i]
        from_x[i].wait_recv()
        block = blocks.at[s_x, t]
        part = blocks.at[s_x, t, :, lower]
        from_da[i] = push(part, part, gd, (0, i), y_peer)
        from_pair[1, i] = push(block, block, gp, (1, i), partner)
        from_y[i].wait_recv()
        block = blocks.at[s_y, t]
        part = blocks.at[s_y, t, :, upper]
        from_db[i] = push(part, part, gd, (1, i), x_peer)
        from_pair[2, i] = push(block, block, gp, (2, i), partner)

    for i in range(1, n_z):
        from_z[i].wait_recv()
        block = blocks.at[me_s, arrive[i]]
        from_x[i] = push(block, block, gxy, (0, i), x_peer)
        from_y[i] = push(block, block, gxy, (1, i), y_peer)
        from_pair[0, i] = push(block, block, gp, (0, i), partner)
        relay_xy(i - 1)

    rows = n_tp * piece
    ff = w_gate.shape[1]
    f_tile, d_tile = 256, min(512, width)
    rp, r1, r2, rz = (rp_s, rp_r), (r1_s, r1_r), (r2_s, r2_r), (rz_s, rz_r)
    send_order = [(me_z + k) % n_z for k in range(1, n_z + 1)]
    back_pair = {}

    def compute(index):
        group = groups[index]
        tokens = blocks[group].reshape(rows, width)

        def up_step(step, _):
            span = pl.ds(pl.multiple_of(step * f_tile, f_tile), f_tile)
            gate_part = jnp.dot(tokens, w_gate[:, span], preferred_element_type=jnp.float32)
            up_part = jnp.dot(tokens, w_up[:, span], preferred_element_type=jnp.float32)
            hidden[:, span] = (gate_part * jax.nn.sigmoid(gate_part) * up_part).astype(jnp.bfloat16)
            return 0

        lax.fori_loop(0, ff // f_tile, up_step, 0)
        share = jnp.transpose(shares_ref[group])
        lane = lax.broadcasted_iota(jnp.int32, share.shape, 1)
        share = jnp.sum(jnp.where(lane == me_s, share, 0.0), axis=1, keepdims=True)
        units = hidden[...]

        def down_step(step, _):
            span = pl.ds(pl.multiple_of(step * d_tile, d_tile), d_tile)
            product = jnp.dot(units, w_down[:, span], preferred_element_type=jnp.float32) * share
            products[index, :, :, span] = product.astype(jnp.bfloat16).reshape(n_tp, piece, d_tile)
            return 0

        lax.fori_loop(0, width // d_tile, down_step, 0)
        for i, z in enumerate(send_order):
            back_pair[index, i] = push(
                products.at[index, z * 2 + 1 - me_c], pair_in.at[index, i], rp, (index, i), partner
            )

    def join(index, i):
        back_pair[index, i].wait_recv()
        joined[index, i] = (
            products[index, send_order[i] * 2 + me_c].astype(jnp.float32)
            + pair_in[index, i].astype(jnp.float32)
        ).astype(jnp.bfloat16)

    own_copy.wait()
    for copy in loads:
        copy.wait()
    for i in range(n_z):
        from_pair[0, i].wait_recv()
    compute(0)
    relay_xy(n_z - 1)
    for i in range(n_z):
        from_pair[1, i].wait_recv()
    compute(1)
    for i in range(n_z):
        t = arrive[i]
        from_da[i].wait_recv()
        part = blocks.at[s_d, t, :, lower]
        from_pair[3, i] = push(part, part, gp, (3, i), partner)
        from_db[i].wait_recv()
        part = blocks.at[s_d, t, :, upper]
        from_pair[4, i] = push(part, part, gp, (4, i), partner)
    first_xs, first_ys = {}, {}
    for i in range(n_z):
        join(1, i)
        first_xs[0, i] = push(
            joined.at[1, i, :, lower], first_x.at[0, i], r1, (0, i), x_peer
        )
    for i in range(n_z):
        from_pair[2, i].wait_recv()
    compute(2)
    for i in range(n_z):
        join(2, i)
        first_ys[0, i] = push(
            joined.at[2, i, :, upper], first_y.at[0, i], r1, (1, i), y_peer
        )
        join(0, i)
    for i in range(n_z):
        from_pair[3, i].wait_recv()
        from_pair[4, i].wait_recv()
    compute(3)
    for i in range(n_z):
        join(3, i)
        first_xs[1, i] = push(
            joined.at[3, i, :, lower], first_x.at[1, i], r1, (2, i), x_peer
        )
        first_ys[1, i] = push(
            joined.at[3, i, :, upper], first_y.at[1, i], r1, (3, i), y_peer
        )
    second_xs, second_ys, back_z = {}, {}, {}
    for i in range(n_z):
        first_xs[1, i].wait_recv()
        relay_a[i] = (
            joined[2, i, :, :half].astype(jnp.float32) + first_x[1, i].astype(jnp.float32)
        ).astype(jnp.bfloat16)
        second_ys[i] = push(relay_a.at[i], second_y.at[i], r2, (0, i), y_peer)
        first_ys[1, i].wait_recv()
        relay_b[i] = (
            joined[1, i, :, half:].astype(jnp.float32) + first_y[1, i].astype(jnp.float32)
        ).astype(jnp.bfloat16)
        second_xs[i] = push(relay_b.at[i], second_x.at[i], r2, (1, i), x_peer)
    for i in range(n_z):
        first_xs[0, i].wait_recv()
        first_ys[0, i].wait_recv()
        second_ys[i].wait_recv()
        second_xs[i].wait_recv()
        low = (
            joined[0, i, :, :half].astype(jnp.float32)
            + first_x[0, i].astype(jnp.float32)
            + second_y[i].astype(jnp.float32)
        )
        high = (
            joined[0, i, :, half:].astype(jnp.float32)
            + first_y[0, i].astype(jnp.float32)
            + second_x[i].astype(jnp.float32)
        )
        column[i] = jnp.concatenate([low, high], axis=1).astype(jnp.bfloat16)
        if i < n_z - 1:
            back_z[i] = push(column.at[i], z_in.at[i], rz, i, z_peers[i])
    total = own_ref[...].astype(jnp.float32) + column[n_z - 1].astype(jnp.float32)
    for i in range(n_z - 1):
        back_z[i].wait_recv()
        total = total + z_in[i].astype(jnp.float32)
    out_ref[...] = total.astype(jnp.bfloat16)
    for copy in sent:
        copy.wait_send()


def dense_local(
    lru_input,
    gate_input,
    documents,
    conv_taps,
    rate_weight,
    inlet_weight,
    decay_param,
    lru_gain,
    out_weight,
    residual,
    ffn_gain,
    routes,
    route_weights,
    w_gate,
    w_up,
    w_down,
):
    n_sp, n_tp = lax.axis_size("sp"), lax.axis_size("tp")
    n_z = n_tp // 2
    rows, channels = lru_input.shape
    width = residual.shape[1]
    ff = w_gate.shape[2]
    piece = rows // n_tp
    padded = -(-n_sp // 8) * 8
    docs = jnp.broadcast_to(documents[:, None], (rows, LANES))
    expert = jnp.arange(padded, dtype=jnp.int32)[:, None]
    shares = jnp.zeros((padded, rows), jnp.float32)
    for k in range(routes.shape[1]):
        shares = shares + jnp.where(
            routes[:, k][None, :] == expert, route_weights[:, k][None, :], 0.0
        )
    vmem = pl.BlockSpec(memory_space=pltpu.VMEM)
    hbm = pl.BlockSpec(memory_space=pl.ANY)
    bf16, f32 = jnp.bfloat16, jnp.float32
    dma = pltpu.SemaphoreType.DMA
    own, normed, all_shares = pl.pallas_call(
        functools.partial(front_kernel, n_sp, n_tp),
        out_shape=(
            jax.ShapeDtypeStruct((piece, width), bf16),
            jax.ShapeDtypeStruct((piece, width), bf16),
            jax.ShapeDtypeStruct((n_sp, padded, rows), f32),
        ),
        in_specs=[vmem] * 9 + [hbm] + [vmem] * 2,
        out_specs=(vmem,) * 3,
        scratch_shapes=[
            pltpu.VMEM((16, channels), bf16),
            pltpu.VMEM((8, LANES), jnp.int32),
            pltpu.VMEM((8, channels), f32),
            pltpu.VMEM((n_sp, 8, channels), f32),
            pltpu.VMEM((n_sp, padded, rows), f32),
            pltpu.VMEM((rows, channels), f32),
            pltpu.VMEM((rows, channels), f32),
            pltpu.VMEM((n_tp, piece, width), bf16),
            pltpu.VMEM((n_z, piece, width), bf16),
            pltpu.VMEM((n_z, piece, width), bf16),
            pltpu.VMEM((n_z, piece, width), bf16),
            pltpu.VMEM((n_tp, piece, LANES), f32),
            pltpu.VMEM((n_z, piece, LANES), f32),
            pltpu.VMEM((n_z, piece, LANES), f32),
            pltpu.VMEM((n_z, piece, LANES), f32),
            pltpu.VMEM((piece, width), bf16),
            dma,
            dma((2,)),
            dma((2,)),
            dma((n_sp,)),
            dma((n_sp,)),
            dma((n_sp,)),
            dma((n_sp,)),
            dma((2, n_z)),
            dma((2, n_z)),
            dma((2, n_z)),
            dma((2, n_z)),
        ],
        compiler_params=pltpu.CompilerParams(
            collective_id=0, has_side_effects=True, vmem_limit_bytes=40 * 2**20
        ),
    )(
        lru_input,
        gate_input,
        docs,
        conv_taps,
        rate_weight,
        inlet_weight,
        decay_param[None, :],
        lru_gain[None, :],
        out_weight,
        residual,
        ffn_gain[None, :],
        shares,
    )
    half = width // 2
    return pl.pallas_call(
        functools.partial(expert_kernel, n_sp, n_tp),
        out_shape=jax.ShapeDtypeStruct((piece, width), bf16),
        in_specs=[vmem] * 3 + [hbm] * 3,
        out_specs=vmem,
        scratch_shapes=[
            pltpu.VMEM((width, ff), bf16),
            pltpu.VMEM((width, ff), bf16),
            pltpu.VMEM((ff, width), bf16),
            pltpu.VMEM((n_sp, n_tp, piece, width), bf16),
            pltpu.VMEM((rows, ff), bf16),
            pltpu.VMEM((n_sp, n_tp, piece, width), bf16),
            pltpu.VMEM((n_sp, n_z, piece, width), bf16),
            pltpu.VMEM((n_sp, n_z, piece, width), bf16),
            pltpu.VMEM((2, n_z, piece, half), bf16),
            pltpu.VMEM((2, n_z, piece, half), bf16),
            pltpu.VMEM((n_z, piece, half), bf16),
            pltpu.VMEM((n_z, piece, half), bf16),
            pltpu.VMEM((n_z, piece, half), bf16),
            pltpu.VMEM((n_z, piece, half), bf16),
            pltpu.VMEM((n_z, piece, width), bf16),
            pltpu.VMEM((n_z, piece, width), bf16),
            dma((3,)),
            dma,
            dma((n_z,)),
            dma((n_z,)),
            dma((2, n_z)),
            dma((2, n_z)),
            dma((2, n_z)),
            dma((2, n_z)),
            dma((5, n_z)),
            dma((5, n_z)),
            dma((4, n_z)),
            dma((4, n_z)),
            dma((4, n_z)),
            dma((4, n_z)),
            dma((2, n_z)),
            dma((2, n_z)),
            dma((n_z,)),
            dma((n_z,)),
        ],
        compiler_params=pltpu.CompilerParams(
            collective_id=1, has_side_effects=True, vmem_limit_bytes=60 * 2**20
        ),
    )(normed, own, all_shares, w_gate[0], w_up[0], w_down[0])


def solution(mesh):
    n_sp, n_tp = mesh.shape["sp"], mesh.shape["tp"]
    body = dense_local if n_sp == 4 and n_tp % 2 == 0 else local
    return jax.shard_map(
        body,
        mesh=mesh,
        in_specs=(
            P("sp", "tp"),
            P("sp", "tp"),
            P("sp"),
            P(None, "tp"),
            P("tp", None, None),
            P("tp", None, None),
            P("tp"),
            P("tp"),
            P("tp", None),
            P("sp", None),
            P(),
            P("sp", None),
            P("sp", None),
            P("sp", None, "tp"),
            P("sp", None, "tp"),
            P("sp", "tp", None),
        ),
        out_specs=P(("sp", "tp"), None),
        check_vma=False,
    )
```

```python
import functools

import jax
import jax.numpy as jnp
from jax import lax
from jax.experimental import pallas as pl
from jax.experimental.pallas import tpu as pltpu
from jax.sharding import PartitionSpec as P

D_RNN = 2048


EPSILON = 1e-06
RATE_SCALE = 8.0


def shifted(block, axis, distance):
    devices = range(lax.axis_size(axis))
    route = [(i - distance, i) for i in devices if i - distance in devices]
    return lax.ppermute(block, axis, route)


def carried_in(value, axis, join, neutral):
    count, mine = (lax.axis_size(axis), lax.axis_index(axis))
    pieces = jax.tree.map(lambda part: lax.all_gather(part, axis), value)
    so_far = jax.tree.map(
        lambda part, zero: jnp.full_like(part, 0) + jnp.asarray(zero, part.dtype), value, neutral
    )

    def hop(position, so_far):
        longer = join(so_far, jax.tree.map(lambda part: part[position], pieces))
        return jax.tree.map(lambda new, old: jnp.where(position < mine, new, old), longer, so_far)

    return lax.fori_loop(0, count - 1, hop, so_far)


def join_runs(earlier_run, later_run):
    return (earlier_run[0] * later_run[0], later_run[0] * earlier_run[1] + later_run[1])


def slot_targets(route_block, expert_count, capacity):
    flat_routes = route_block.reshape(-1)
    onehot = (flat_routes[:, None] == jnp.arange(expert_count, dtype=jnp.int32)[None, :]).astype(
        jnp.int32
    )
    earlier_hits = jnp.cumsum(onehot, axis=0) - onehot
    slot_index = jnp.sum(earlier_hits * onehot, axis=1)
    return (flat_routes * capacity + slot_index).reshape(route_block.shape)


def pick_matrix(targets, slot_total):
    slot_hits = targets[None, :, :] == jnp.arange(slot_total, dtype=jnp.int32)[:, None, None]
    return jnp.sum(slot_hits.astype(jnp.int32), axis=2).astype(jnp.bfloat16)


def rms_rows(row_block, gain_vector):
    floated = row_block.astype(jnp.float32)
    inverse_rms = lax.rsqrt(jnp.mean(floated * floated, axis=1, keepdims=True) + EPSILON)
    return (floated * inverse_rms * gain_vector[None, :]).astype(jnp.bfloat16)


def expert_apply(row_piece, gate_weight, up_weight, down_weight):
    gate_part = jnp.dot(row_piece, gate_weight, preferred_element_type=jnp.float32)
    up_part = jnp.dot(row_piece, up_weight, preferred_element_type=jnp.float32)
    hidden_units = (jax.nn.silu(gate_part) * up_part).astype(jnp.bfloat16)
    return jnp.dot(hidden_units, down_weight, preferred_element_type=jnp.float32)


def local(
    lru_input,
    gate_input,
    documents,
    conv_taps,
    rate_weight,
    inlet_weight,
    decay_param,
    lru_gain,
    out_weight,
    residual,
    ffn_gain,
    routes,
    route_weights,
    w_gate,
    w_up,
    w_down,
):
    positions = lru_input.shape[0]
    channels = lru_input.shape[1]
    model_width = residual.shape[1]
    reach_back = conv_taps.shape[0] - 1
    tail_rows, tail_docs = shifted(
        (lru_input[positions - reach_back :], documents[positions - reach_back :] + 1), "sp", 1
    )
    prior_docs = jnp.concatenate([tail_docs - 1, documents])
    padded_input = jnp.concatenate([tail_rows, lru_input], axis=0)
    conv_sum = jnp.zeros((positions, channels), jnp.float32)
    for tap_index in range(reach_back + 1):
        same_doc = (prior_docs[tap_index : tap_index + positions] == documents).astype(jnp.float32)[
            :, None
        ]
        conv_sum = (
            conv_sum
            + padded_input[tap_index : tap_index + positions].astype(jnp.float32)
            * conv_taps[tap_index].astype(jnp.float32)[None, :]
            * same_doc
        )
    convolved = conv_sum.astype(jnp.bfloat16)
    grouped = convolved.reshape(positions, rate_weight.shape[0], rate_weight.shape[1])
    rate_gate = jax.nn.sigmoid(
        jnp.einsum(
            "tnc,ncd->tnd", grouped, rate_weight, preferred_element_type=jnp.float32
        ).reshape(positions, channels)
    )
    inlet_gate = jax.nn.sigmoid(
        jnp.einsum(
            "tnc,ncd->tnd", grouped, inlet_weight, preferred_element_type=jnp.float32
        ).reshape(positions, channels)
    )
    log_decay = -RATE_SCALE * rate_gate * jax.nn.softplus(-decay_param)[None, :]
    starts = (prior_docs[reach_back - 1 : reach_back - 1 + positions] != documents)[:, None]
    decay_step = jnp.where(starts, 0.0, jnp.exp(log_decay))
    norm_factor = jnp.where(starts, 1.0, jnp.sqrt(-jnp.expm1(2.0 * log_decay)))
    drive_term = norm_factor * inlet_gate * convolved.astype(jnp.float32)
    decay_run, local_state = lax.associative_scan(join_runs, (decay_step, drive_term), axis=0)
    carried = carried_in(
        (decay_run[positions - 1], local_state[positions - 1]),
        "sp",
        join_runs,
        (jnp.ones((channels,), jnp.float32), jnp.zeros((channels,), jnp.float32)),
    )
    hidden_state = local_state + decay_run * carried[1][None, :]
    square_sums = lax.psum(jnp.sum(hidden_state * hidden_state, axis=1), "tp")
    inverse_rms = lax.rsqrt(square_sums[:, None] / D_RNN + EPSILON)
    mixer_rows = (
        hidden_state * inverse_rms * lru_gain[None, :] * jax.nn.gelu(gate_input.astype(jnp.float32))
    ).astype(jnp.bfloat16)
    tp_count = lax.axis_size("tp")
    tp_here = lax.axis_index("tp")
    expert_count = lax.axis_size("sp")
    route_rows = positions // tp_count
    top_count = routes.shape[1]
    capacity = 2 * top_count * route_rows // expert_count
    slot_total = expert_count * capacity
    projected = lax.psum_scatter(
        jnp.dot(mixer_rows, out_weight, preferred_element_type=jnp.float32).astype(jnp.bfloat16),
        "tp",
        scatter_dimension=0,
        tiled=True,
    ).astype(jnp.float32)
    own_rows = (
        lax.dynamic_slice_in_dim(residual, tp_here * route_rows, route_rows, 0).astype(jnp.float32)
        + projected
    ).astype(jnp.bfloat16)
    own_routes = lax.dynamic_slice_in_dim(routes, tp_here * route_rows, route_rows, 0)
    targets = slot_targets(own_routes, expert_count, capacity)
    outgoing = jnp.dot(
        pick_matrix(targets, slot_total),
        rms_rows(own_rows, ffn_gain),
        preferred_element_type=jnp.float32,
    ).astype(jnp.bfloat16)
    arrived = lax.all_to_all(
        outgoing.reshape(expert_count, capacity, model_width),
        "sp",
        split_axis=0,
        concat_axis=0,
        tiled=True,
    )
    partial_out = expert_apply(
        lax.all_gather(arrived.reshape(slot_total, model_width), "tp", axis=0, tiled=True),
        w_gate[0],
        w_up[0],
        w_down[0],
    )
    expert_out = lax.psum_scatter(
        partial_out.astype(jnp.bfloat16), "tp", scatter_dimension=0, tiled=True
    )
    returned = lax.all_to_all(
        expert_out.reshape(expert_count, capacity, model_width),
        "sp",
        split_axis=0,
        concat_axis=0,
        tiled=True,
    )
    picked = returned.reshape(slot_total, model_width)[targets.reshape(-1)].astype(jnp.float32)
    picked = picked.reshape(route_rows, top_count, model_width)
    own_weights = lax.dynamic_slice_in_dim(route_weights, tp_here * route_rows, route_rows, 0)
    routed = jnp.sum(picked * own_weights[:, :, None], axis=1)
    return (own_rows.astype(jnp.float32) + routed).astype(jnp.bfloat16)


MESH = pl.DeviceIdType.MESH
LANES = 128
GELU_SCALE = 0.7978845608028654


def sender(source, target, send_sem, recv_sem, peer):
    return pltpu.make_async_remote_copy(
        src_ref=source,
        dst_ref=target,
        send_sem=send_sem,
        recv_sem=recv_sem,
        device_id=peer,
        device_id_type=MESH,
    )


def greet(peers):
    barrier = pltpu.get_barrier_semaphore()
    for peer in peers:
        pl.semaphore_signal(barrier, inc=1, device_id=peer, device_id_type=MESH)
    pl.semaphore_wait(barrier, len(peers))


def one_minus_exp(value):
    series = 1.0 + value * (1.0 / 6.0)
    for order in (5.0, 4.0, 3.0, 2.0):
        series = 1.0 + value * (1.0 / order) * series
    return jnp.where(value > -0.25, -value * series, 1.0 - jnp.exp(value))


def down_by(block, distance, filler):
    count = block.shape[0]
    if distance % 8 == 0:
        top = jnp.full((distance, block.shape[1]), filler, block.dtype)
        return jnp.concatenate([top, block[: count - distance]], axis=0)
    row = lax.broadcasted_iota(jnp.int32, block.shape, 0)
    return jnp.where(row >= distance, pltpu.roll(block, distance, 0), filler)


LATE = 8


def layer_kernel(
    n_sp,
    n_tp,
    lru_hbm,
    gate_hbm,
    docs_hbm,
    taps_hbm,
    rate_hbm,
    inlet_hbm,
    decay_hbm,
    gain_hbm,
    out_w_hbm,
    residual_hbm,
    ffn_hbm,
    routes_hbm,
    shares_hbm,
    w_gate_hbm,
    w_up_hbm,
    w_down_hbm,
    out_ref,
    lru_ref,
    gate_ref,
    docs_row,
    taps_ref,
    rate_ref,
    inlet_ref,
    decay_ref,
    gain_ref,
    out_w_ref,
    ffn_ref,
    routes_ref,
    route_w_ref,
    docs_ref,
    weights_ref,
    halo_x,
    halo_d,
    carry_out,
    carry_in,
    share_in,
    run_a,
    run_b,
    parts,
    pair_in,
    z_out,
    z_in,
    squares,
    square_pair,
    square_out,
    square_in,
    res_rows,
    own_ref,
    normed_ref,
    w_gate,
    w_up,
    w_down,
    share_cols,
    blocks,
    hidden_units,
    products,
    back_in,
    joined,
    first_x,
    first_y,
    second_x,
    second_y,
    relay_a,
    relay_b,
    column,
    last_in,
    load_sem,
    res_sem,
    w_sem,
    own_sem,
    halo_s,
    halo_r,
    carry_s,
    carry_r,
    share_s,
    share_r,
    pair_s,
    pair_r,
    z_s,
    z_r,
    gz_s,
    gz_r,
    gxy_s,
    gxy_r,
    gd_s,
    gd_r,
    gp_s,
    gp_r,
    rp_s,
    rp_r,
    r1_s,
    r1_r,
    r2_s,
    r2_r,
    rz_s,
    rz_r,
):
    me_s, me_t = lax.axis_index("sp"), lax.axis_index("tp")
    n_z = n_tp // 2
    me_z, me_c = me_t // 2, me_t % 2
    rows, channels = lru_ref.shape
    width = out_w_ref.shape[1]
    piece = rows // n_tp
    pairs = (
        (lru_hbm, lru_ref),
        (docs_hbm, docs_row),
        (taps_hbm, taps_ref),
        (rate_hbm, rate_ref),
        (inlet_hbm, inlet_ref),
        (decay_hbm, decay_ref),
        (routes_hbm, routes_ref),
        (shares_hbm, route_w_ref),
        (out_w_hbm, out_w_ref),
        (gate_hbm, gate_ref),
        (gain_hbm, gain_ref),
        (ffn_hbm, ffn_ref),
    )
    loads = [
        pltpu.make_async_copy(source, target, load_sem.at[k])
        for k, (source, target) in enumerate(pairs)
    ]
    for copy in loads:
        copy.start()
    residual_copy = pltpu.make_async_copy(
        residual_hbm.at[pl.ds(pl.multiple_of(me_t * piece, piece), piece)], res_rows, res_sem
    )
    residual_copy.start()
    w_loads = [
        pltpu.make_async_copy(source, target, w_sem.at[k])
        for k, (source, target) in enumerate(
            ((w_gate_hbm, w_gate), (w_up_hbm, w_up), (w_down_hbm, w_down))
        )
    ]
    for copy in w_loads:
        copy.start()
    s_x = me_s + 1 - 2 * (me_s % 2)
    s_y = (me_s + 2) % n_sp
    s_d = n_sp - 1 - me_s
    x_peer, y_peer = (s_x, me_t), (s_y, me_t)
    partner = (me_s, me_z * 2 + 1 - me_c)
    sp_peers = [((me_s + k) % n_sp, me_t) for k in range(1, n_sp)]
    z_peers = [(me_s, ((me_z + k) % n_z) * 2 + me_c) for k in range(1, n_z)]
    greet(sp_peers + z_peers + [partner])
    loads[0].wait()
    loads[1].wait()
    docs = jnp.transpose(jnp.broadcast_to(docs_row[...], (8, rows)))
    docs = jnp.broadcast_to(docs[:, :1], (rows, LANES))
    docs_ref[...] = docs
    halo = [
        sender(lru_ref.at[pl.ds(rows - 16, 16)], halo_x, halo_s.at[0], halo_r.at[0], sp_peers[0]),
        sender(docs_ref.at[pl.ds(rows - 8, 8)], halo_d, halo_s.at[1], halo_r.at[1], sp_peers[0]),
    ]
    for copy in halo:
        copy.start()
    loads[6].wait()
    loads[7].wait()
    expert = lax.broadcasted_iota(jnp.int32, weights_ref.shape, 0)
    shares = jnp.zeros(weights_ref.shape, jnp.float32)
    for k in range(routes_ref.shape[0]):
        shares = shares + jnp.where(
            routes_ref[k : k + 1] == expert, route_w_ref[k : k + 1], 0.0
        )
    weights_ref[...] = shares
    share = [
        sender(weights_ref, share_in.at[me_s], share_s.at[k], share_r.at[k], peer)
        for k, peer in enumerate(sp_peers)
    ]
    for copy in share:
        copy.start()
    share_in[pl.ds(me_s, 1)] = shares[None]
    for k in (2, 3, 4, 5, 9, 10, 11):
        loads[k].wait()
    for copy in halo:
        copy.wait()

    before = jnp.where(me_s == 0, jnp.int32(-1), halo_d[...])
    docs_long = jnp.concatenate([before, docs], axis=0)
    taps = taps_ref[...].astype(jnp.float32)
    starts = docs_long[7 : 7 + rows] != docs
    for group in range(channels // LANES):
        span = slice(group * LANES, (group + 1) * LANES)
        long = jnp.concatenate(
            [halo_x[:, span].astype(jnp.float32)[8:], lru_ref[:, span].astype(jnp.float32)], axis=0
        )
        total = jnp.zeros((rows, LANES), jnp.float32)
        for tap in range(taps.shape[0]):
            first = 8 - (taps.shape[0] - 1) + tap
            same = docs_long[first : first + rows] == docs
            total = total + jnp.where(same, long[first : first + rows], 0.0) * taps[tap : tap + 1, span]
        convolved = total.astype(jnp.bfloat16)
        rate = jax.nn.sigmoid(
            jnp.dot(convolved, rate_ref[group], preferred_element_type=jnp.float32)
        )
        inlet = jax.nn.sigmoid(
            jnp.dot(convolved, inlet_ref[group], preferred_element_type=jnp.float32)
        )
        minus = -decay_ref[:, span]
        soft = jnp.maximum(minus, 0.0) + jnp.log1p(jnp.exp(-jnp.abs(minus)))
        log_decay = -RATE_SCALE * rate * soft
        step = jnp.where(starts, 0.0, jnp.exp(log_decay))
        factor = jnp.where(starts, 1.0, jnp.sqrt(one_minus_exp(2.0 * log_decay)))
        state = factor * inlet * convolved.astype(jnp.float32)
        distance = 1
        while distance < rows:
            state = state + step * down_by(state, distance, 0.0)
            step = step * down_by(step, distance, 1.0)
            distance *= 2
        run_a[:, span] = step
        run_b[:, span] = state
        carry_out[:, span] = jnp.concatenate(
            [step[rows - 1 :], state[rows - 1 :], jnp.zeros((6, LANES), jnp.float32)], axis=0
        )
    carry = [
        sender(carry_out, carry_in.at[me_s], carry_s.at[k], carry_r.at[k], peer)
        for k, peer in enumerate(sp_peers)
    ]
    for copy in carry:
        copy.start()
    carry_in[pl.ds(me_s, 1)] = carry_out[...][None]
    raw = gate_ref[...].astype(jnp.float32)
    gelu = 0.5 * raw * (1.0 + jnp.tanh(GELU_SCALE * (raw + 0.044715 * raw * raw * raw)))
    gelu = gelu * gain_ref[...]
    for copy in carry:
        copy.wait()
    carried = jnp.zeros((1, channels), jnp.float32)
    for place in range(n_sp - 1):
        tile = carry_in[place]
        carried = jnp.where(place < me_s, tile[1:2] + tile[0:1] * carried, carried)
    hidden = run_b[...] + run_a[...] * carried
    row_squares = jnp.sum(hidden * hidden, axis=1, keepdims=True)
    squares[...] = jnp.broadcast_to(row_squares, (rows, LANES)).reshape(n_tp, piece, LANES)
    loads[LATE].wait()
    mixer = (hidden * gelu).astype(jnp.bfloat16)
    tile_width = min(512, width)
    for first in range(0, width, tile_width):
        span = slice(first, first + tile_width)
        product = jnp.dot(mixer, out_w_ref[:, span], preferred_element_type=jnp.float32)
        parts[:, :, span] = product.astype(jnp.bfloat16).reshape(n_tp, piece, tile_width)

    order = [(me_z + k) % n_z for k in range(1, n_z + 1)]
    pair = []
    for i, z in enumerate(order):
        theirs = z * 2 + 1 - me_c
        pair.append(
            (
                sender(parts.at[theirs], pair_in.at[i], pair_s.at[0, i], pair_r.at[0, i], partner),
                sender(
                    squares.at[theirs], square_pair.at[i], pair_s.at[1, i], pair_r.at[1, i], partner
                ),
            )
        )
        for copy in pair[-1]:
            copy.start()
    z_copies = []
    for i, z in enumerate(order):
        mine = z * 2 + me_c
        for copy in pair[i]:
            copy.wait_recv()
        z_out[i] = (
            parts[mine].astype(jnp.float32) + pair_in[i].astype(jnp.float32)
        ).astype(jnp.bfloat16)
        square_out[i] = squares[mine] + square_pair[i]
        if i < n_z - 1:
            peer = (me_s, mine)
            copies = (
                sender(z_out.at[i], z_in.at[i], z_s.at[0, i], z_r.at[0, i], peer),
                sender(square_out.at[i], square_in.at[i], z_s.at[1, i], z_r.at[1, i], peer),
            )
            for copy in copies:
                copy.start()
            z_copies.append(copies)
    summed = z_out[n_z - 1].astype(jnp.float32)
    square_sum = square_out[n_z - 1]
    for i in range(n_z - 1):
        for copy in z_copies[i]:
            copy.wait_recv()
        summed = summed + z_in[i].astype(jnp.float32)
        square_sum = square_sum + square_in[i]
    inverse = lax.rsqrt(square_sum[:, :1] / (channels * n_tp) + EPSILON)
    residual_copy.wait()
    own = (res_rows[...].astype(jnp.float32) + summed * inverse).astype(jnp.bfloat16)
    own_ref[...] = own
    floated = own.astype(jnp.float32)
    inverse = lax.rsqrt(jnp.mean(floated * floated, axis=1, keepdims=True) + EPSILON)
    normed_ref[...] = (floated * inverse * ffn_ref[...]).astype(jnp.bfloat16)

    half = width // 2
    lower, upper = pl.ds(0, half), pl.ds(half, half)
    sent = []

    def push(source, target, sems, slot, peer):
        copy = sender(source, target, sems[0].at[slot], sems[1].at[slot], peer)
        copy.start()
        sent.append(copy)
        return copy

    gz, gxy, gd, gp = (gz_s, gz_r), (gxy_s, gxy_r), (gd_s, gd_r), (gp_s, gp_r)
    rp, r1, r2, rz = (rp_s, rp_r), (r1_s, r1_r), (r2_s, r2_r), (rz_s, rz_r)
    from_z, from_x, from_y, from_da, from_db, from_pair = {}, {}, {}, {}, {}, {}

    def spread(i):
        block = blocks.at[i, me_s, me_c]
        if i == 0:
            source = normed_ref
        else:
            from_z[i].wait_recv()
            source = block
        from_x[i] = push(source, block, gxy, (0, i), x_peer)
        from_y[i] = push(source, block, gxy, (1, i), y_peer)
        from_pair[0, i] = push(source, block, gp, (0, i), partner)

    def relay(i):
        from_x[i].wait_recv()
        block, part = blocks.at[i, s_x, me_c], blocks.at[i, s_x, me_c, :, lower]
        from_da[i] = push(part, part, gd, (0, i), y_peer)
        from_pair[1, i] = push(block, block, gp, (1, i), partner)
        from_y[i].wait_recv()
        block, part = blocks.at[i, s_y, me_c], blocks.at[i, s_y, me_c, :, upper]
        from_db[i] = push(part, part, gd, (1, i), x_peer)
        from_pair[2, i] = push(block, block, gp, (2, i), partner)

    def hand_over(i):
        from_da[i].wait_recv()
        part = blocks.at[i, s_d, me_c, :, lower]
        from_pair[3, i] = push(part, part, gp, (3, i), partner)
        from_db[i].wait_recv()
        part = blocks.at[i, s_d, me_c, :, upper]
        from_pair[4, i] = push(part, part, gp, (4, i), partner)

    own_copy = pltpu.make_async_copy(normed_ref, blocks.at[0, me_s, me_c], own_sem)
    own_copy.start()
    spread(0)
    for k in range(n_z - 1):
        from_z[k + 1] = push(normed_ref, blocks.at[k + 1, me_s, me_c], gz, k, z_peers[k])
    for copy in share:
        copy.wait()
    for place in range(n_sp):
        turned = jnp.transpose(share_in[place])
        lane = lax.broadcasted_iota(jnp.int32, turned.shape, 1)
        chosen = jnp.sum(jnp.where(lane == me_s, turned, 0.0), axis=1, keepdims=True)
        share_cols[place] = jnp.broadcast_to(chosen, (rows, LANES))

    ff = w_gate.shape[1]
    f_tile, d_tile = 256, min(512, width)
    count = n_sp * 2 * piece
    back, first_xs, first_ys, second_xs, second_ys, back_z = {}, {}, {}, {}, {}, {}

    def rise(i):
        for k in range(5):
            from_pair[k, i].wait_recv()
        tokens = blocks[i].reshape(count, width)

        def up_step(step, _):
            span = pl.ds(pl.multiple_of(step * f_tile, f_tile), f_tile)
            gate_part = jnp.dot(tokens, w_gate[:, span], preferred_element_type=jnp.float32)
            up_part = jnp.dot(tokens, w_up[:, span], preferred_element_type=jnp.float32)
            hidden_units[:, span] = (gate_part * jax.nn.sigmoid(gate_part) * up_part).astype(
                jnp.bfloat16
            )
            return 0

        lax.fori_loop(0, ff // f_tile, up_step, 0)

    def fall(i):
        z = (me_z + n_z - i) % n_z
        first = pl.multiple_of(z * (2 * piece), 2 * piece)
        scale = share_cols[:, pl.ds(first, 2 * piece), :].reshape(count, LANES)[:, :1]
        units = hidden_units[...]

        def down_step(step, _):
            span = pl.ds(pl.multiple_of(step * d_tile, d_tile), d_tile)
            product = jnp.dot(units, w_down[:, span], preferred_element_type=jnp.float32) * scale
            products[i, :, :, :, span] = product.astype(jnp.bfloat16).reshape(
                n_sp, 2, piece, d_tile
            )
            return 0

        lax.fori_loop(0, width // d_tile, down_step, 0)
        for k, group in enumerate((s_d, s_x, s_y, me_s)):
            back[k, i] = push(
                products.at[i, group, 1 - me_c], back_in.at[i, k], rp, (k, i), partner
            )

    def join(i):
        for k, group in enumerate((s_d, s_x, s_y, me_s)):
            back[k, i].wait_recv()
            joined[i, k] = (
                products[i, group, me_c].astype(jnp.float32) + back_in[i, k].astype(jnp.float32)
            ).astype(jnp.bfloat16)
            if k == 0:
                first_xs[1, i] = push(
                    joined.at[i, 0, :, lower], first_x.at[1, i], r1, (2, i), x_peer
                )
                first_ys[1, i] = push(
                    joined.at[i, 0, :, upper], first_y.at[1, i], r1, (3, i), y_peer
                )
            elif k == 1:
                first_xs[0, i] = push(
                    joined.at[i, 1, :, lower], first_x.at[0, i], r1, (0, i), x_peer
                )
            elif k == 2:
                first_ys[0, i] = push(
                    joined.at[i, 2, :, upper], first_y.at[0, i], r1, (1, i), y_peer
                )

    def turn(i):
        first_xs[1, i].wait_recv()
        relay_a[i] = (
            joined[i, 2, :, :half].astype(jnp.float32) + first_x[1, i].astype(jnp.float32)
        ).astype(jnp.bfloat16)
        second_ys[i] = push(relay_a.at[i], second_y.at[i], r2, (0, i), y_peer)
        first_ys[1, i].wait_recv()
        relay_b[i] = (
            joined[i, 1, :, half:].astype(jnp.float32) + first_y[1, i].astype(jnp.float32)
        ).astype(jnp.bfloat16)
        second_xs[i] = push(relay_b.at[i], second_x.at[i], r2, (1, i), x_peer)

    def finish(i):
        for copies in (first_xs, first_ys):
            copies[0, i].wait_recv()
        for copies in (second_xs, second_ys):
            copies[i].wait_recv()
        low = (
            joined[i, 3, :, :half].astype(jnp.float32)
            + first_x[0, i].astype(jnp.float32)
            + second_y[i].astype(jnp.float32)
        )
        high = (
            joined[i, 3, :, half:].astype(jnp.float32)
            + first_y[0, i].astype(jnp.float32)
            + second_x[i].astype(jnp.float32)
        )
        column[i] = jnp.concatenate([low, high], axis=1).astype(jnp.bfloat16)
        if i > 0:
            peer = (me_s, ((me_z + n_z - i) % n_z) * 2 + me_c)
            back_z[i] = push(column.at[i], last_in.at[i], rz, i, peer)

    own_copy.wait()
    for copy in w_loads:
        copy.wait()
    last = n_z - 1
    for tick in range(-2, n_z + 2):
        plan = (
            (spread, tick + 3),
            (relay, tick + 2),
            (hand_over, tick + 1),
            (rise, tick),
            (join, tick - 1),
            (finish, tick - 2),
            (fall, tick),
            (turn, tick - 1),
        )
        for stage, i in plan:
            if 0 <= i <= last and not (stage is spread and i == 0):
                stage(i)
    total = own_ref[...].astype(jnp.float32) + column[0].astype(jnp.float32)
    for i in range(1, n_z):
        back_z[i].wait_recv()
        total = total + last_in[i].astype(jnp.float32)
    out_ref[...] = total.astype(jnp.bfloat16)
    for copies in pair + z_copies:
        for copy in copies:
            copy.wait_send()
    for copy in sent:
        copy.wait_send()


def dense_local(
    lru_input,
    gate_input,
    documents,
    conv_taps,
    rate_weight,
    inlet_weight,
    decay_param,
    lru_gain,
    out_weight,
    residual,
    ffn_gain,
    routes,
    route_weights,
    w_gate,
    w_up,
    w_down,
):
    n_sp, n_tp = lax.axis_size("sp"), lax.axis_size("tp")
    n_z = n_tp // 2
    rows, channels = lru_input.shape
    width = residual.shape[1]
    ff = w_gate.shape[2]
    piece = rows // n_tp
    padded = -(-n_sp // 8) * 8
    vmem = pl.BlockSpec(memory_space=pltpu.VMEM)
    half = width // 2
    top = routes.shape[1]
    hbm = pl.BlockSpec(memory_space=pl.ANY)
    bf16, f32 = jnp.bfloat16, jnp.float32
    dma = pltpu.SemaphoreType.DMA
    rows_buffer = pltpu.VMEM((n_z, piece, width), bf16)
    half_buffer = pltpu.VMEM((n_z, piece, half), bf16)
    chunks = pltpu.VMEM((n_z, n_sp, 2, piece, width), bf16)
    groups = pltpu.VMEM((n_z, n_sp, piece, width), bf16)
    square_buffer = pltpu.VMEM((n_z, piece, LANES), f32)
    shapes = (
        [(2,)] * 2
        + [(n_sp,)] * 4
        + [(2, n_z)] * 4
        + [(n_z,)] * 2
        + [(2, n_z)] * 4
        + [(5, n_z)] * 2
        + [(4, n_z)] * 4
        + [(2, n_z)] * 2
        + [(n_z,)] * 2
    )
    return pl.pallas_call(
        functools.partial(layer_kernel, n_sp, n_tp),
        out_shape=jax.ShapeDtypeStruct((piece, width), bf16),
        in_specs=[hbm] * 16,
        out_specs=vmem,
        scratch_shapes=[
            pltpu.VMEM((rows, channels), bf16),
            pltpu.VMEM((rows, channels), bf16),
            pltpu.VMEM((1, rows), jnp.int32),
            pltpu.VMEM(conv_taps.shape, bf16),
            pltpu.VMEM(rate_weight.shape, bf16),
            pltpu.VMEM(inlet_weight.shape, bf16),
            pltpu.VMEM((1, channels), f32),
            pltpu.VMEM((1, channels), f32),
            pltpu.VMEM((channels, width), bf16),
            pltpu.VMEM((1, width), f32),
            pltpu.VMEM((top, rows), jnp.int32),
            pltpu.VMEM((top, rows), f32),
            pltpu.VMEM((rows, LANES), jnp.int32),
            pltpu.VMEM((padded, rows), f32),
            pltpu.VMEM((16, channels), bf16),
            pltpu.VMEM((8, LANES), jnp.int32),
            pltpu.VMEM((8, channels), f32),
            pltpu.VMEM((n_sp, 8, channels), f32),
            pltpu.VMEM((n_sp, padded, rows), f32),
            pltpu.VMEM((rows, channels), f32),
            pltpu.VMEM((rows, channels), f32),
            pltpu.VMEM((n_tp, piece, width), bf16),
            rows_buffer,
            rows_buffer,
            rows_buffer,
            pltpu.VMEM((n_tp, piece, LANES), f32),
            square_buffer,
            square_buffer,
            square_buffer,
            pltpu.VMEM((piece, width), bf16),
            pltpu.VMEM((piece, width), bf16),
            pltpu.VMEM((piece, width), bf16),
            pltpu.VMEM((width, ff), bf16),
            pltpu.VMEM((width, ff), bf16),
            pltpu.VMEM((ff, width), bf16),
            pltpu.VMEM((n_sp, rows, LANES), f32),
            chunks,
            pltpu.VMEM((n_sp * 2 * piece, ff), bf16),
            chunks,
            groups,
            groups,
            pltpu.VMEM((2, n_z, piece, half), bf16),
            pltpu.VMEM((2, n_z, piece, half), bf16),
            half_buffer,
            half_buffer,
            half_buffer,
            half_buffer,
            rows_buffer,
            rows_buffer,
            dma((12,)),
            dma,
            dma((3,)),
            dma,
        ]
        + [dma(shape) for shape in shapes],
        compiler_params=pltpu.CompilerParams(
            collective_id=0, has_side_effects=True, vmem_limit_bytes=60 * 2**20
        ),
    )(
        lru_input,
        gate_input,
        documents[None, :],
        conv_taps,
        rate_weight,
        inlet_weight,
        decay_param[None, :],
        lru_gain[None, :],
        out_weight,
        residual,
        ffn_gain[None, :],
        routes.T,
        route_weights.T,
        w_gate[0],
        w_up[0],
        w_down[0],
    )


def solution(mesh):
    n_sp, n_tp = mesh.shape["sp"], mesh.shape["tp"]
    body = dense_local if n_sp == 4 and n_tp % 2 == 0 else local
    return jax.shard_map(
        body,
        mesh=mesh,
        in_specs=(
            P("sp", "tp"),
            P("sp", "tp"),
            P("sp"),
            P(None, "tp"),
            P("tp", None, None),
            P("tp", None, None),
            P("tp"),
            P("tp"),
            P("tp", None),
            P("sp", None),
            P(),
            P("sp", None),
            P("sp", None),
            P("sp", None, "tp"),
            P("sp", None, "tp"),
            P("sp", "tp", None),
        ),
        out_specs=P(("sp", "tp"), None),
        check_vma=False,
    )
```

```python
import functools

import jax
import jax.numpy as jnp
from jax import lax
from jax.experimental import pallas as pl
from jax.experimental.pallas import tpu as pltpu
from jax.sharding import PartitionSpec as P

D_RNN = 2048


EPSILON = 1e-06
RATE_SCALE = 8.0


def shifted(block, axis, distance):
    devices = range(lax.axis_size(axis))
    route = [(i - distance, i) for i in devices if i - distance in devices]
    return lax.ppermute(block, axis, route)


def carried_in(value, axis, join, neutral):
    count, mine = (lax.axis_size(axis), lax.axis_index(axis))
    pieces = jax.tree.map(lambda part: lax.all_gather(part, axis), value)
    so_far = jax.tree.map(
        lambda part, zero: jnp.full_like(part, 0) + jnp.asarray(zero, part.dtype), value, neutral
    )

    def hop(position, so_far):
        longer = join(so_far, jax.tree.map(lambda part: part[position], pieces))
        return jax.tree.map(lambda new, old: jnp.where(position < mine, new, old), longer, so_far)

    return lax.fori_loop(0, count - 1, hop, so_far)


def join_runs(earlier_run, later_run):
    return (earlier_run[0] * later_run[0], later_run[0] * earlier_run[1] + later_run[1])


def slot_targets(route_block, expert_count, capacity):
    flat_routes = route_block.reshape(-1)
    onehot = (flat_routes[:, None] == jnp.arange(expert_count, dtype=jnp.int32)[None, :]).astype(
        jnp.int32
    )
    earlier_hits = jnp.cumsum(onehot, axis=0) - onehot
    slot_index = jnp.sum(earlier_hits * onehot, axis=1)
    return (flat_routes * capacity + slot_index).reshape(route_block.shape)


def pick_matrix(targets, slot_total):
    slot_hits = targets[None, :, :] == jnp.arange(slot_total, dtype=jnp.int32)[:, None, None]
    return jnp.sum(slot_hits.astype(jnp.int32), axis=2).astype(jnp.bfloat16)


def rms_rows(row_block, gain_vector):
    floated = row_block.astype(jnp.float32)
    inverse_rms = lax.rsqrt(jnp.mean(floated * floated, axis=1, keepdims=True) + EPSILON)
    return (floated * inverse_rms * gain_vector[None, :]).astype(jnp.bfloat16)


def expert_apply(row_piece, gate_weight, up_weight, down_weight):
    gate_part = jnp.dot(row_piece, gate_weight, preferred_element_type=jnp.float32)
    up_part = jnp.dot(row_piece, up_weight, preferred_element_type=jnp.float32)
    hidden_units = (jax.nn.silu(gate_part) * up_part).astype(jnp.bfloat16)
    return jnp.dot(hidden_units, down_weight, preferred_element_type=jnp.float32)


def local(
    lru_input,
    gate_input,
    documents,
    conv_taps,
    rate_weight,
    inlet_weight,
    decay_param,
    lru_gain,
    out_weight,
    residual,
    ffn_gain,
    routes,
    route_weights,
    w_gate,
    w_up,
    w_down,
):
    positions = lru_input.shape[0]
    channels = lru_input.shape[1]
    model_width = residual.shape[1]
    reach_back = conv_taps.shape[0] - 1
    tail_rows, tail_docs = shifted(
        (lru_input[positions - reach_back :], documents[positions - reach_back :] + 1), "sp", 1
    )
    prior_docs = jnp.concatenate([tail_docs - 1, documents])
    padded_input = jnp.concatenate([tail_rows, lru_input], axis=0)
    conv_sum = jnp.zeros((positions, channels), jnp.float32)
    for tap_index in range(reach_back + 1):
        same_doc = (prior_docs[tap_index : tap_index + positions] == documents).astype(jnp.float32)[
            :, None
        ]
        conv_sum = (
            conv_sum
            + padded_input[tap_index : tap_index + positions].astype(jnp.float32)
            * conv_taps[tap_index].astype(jnp.float32)[None, :]
            * same_doc
        )
    convolved = conv_sum.astype(jnp.bfloat16)
    grouped = convolved.reshape(positions, rate_weight.shape[0], rate_weight.shape[1])
    rate_gate = jax.nn.sigmoid(
        jnp.einsum(
            "tnc,ncd->tnd", grouped, rate_weight, preferred_element_type=jnp.float32
        ).reshape(positions, channels)
    )
    inlet_gate = jax.nn.sigmoid(
        jnp.einsum(
            "tnc,ncd->tnd", grouped, inlet_weight, preferred_element_type=jnp.float32
        ).reshape(positions, channels)
    )
    log_decay = -RATE_SCALE * rate_gate * jax.nn.softplus(-decay_param)[None, :]
    starts = (prior_docs[reach_back - 1 : reach_back - 1 + positions] != documents)[:, None]
    decay_step = jnp.where(starts, 0.0, jnp.exp(log_decay))
    norm_factor = jnp.where(starts, 1.0, jnp.sqrt(-jnp.expm1(2.0 * log_decay)))
    drive_term = norm_factor * inlet_gate * convolved.astype(jnp.float32)
    decay_run, local_state = lax.associative_scan(join_runs, (decay_step, drive_term), axis=0)
    carried = carried_in(
        (decay_run[positions - 1], local_state[positions - 1]),
        "sp",
        join_runs,
        (jnp.ones((channels,), jnp.float32), jnp.zeros((channels,), jnp.float32)),
    )
    hidden_state = local_state + decay_run * carried[1][None, :]
    square_sums = lax.psum(jnp.sum(hidden_state * hidden_state, axis=1), "tp")
    inverse_rms = lax.rsqrt(square_sums[:, None] / D_RNN + EPSILON)
    mixer_rows = (
        hidden_state * inverse_rms * lru_gain[None, :] * jax.nn.gelu(gate_input.astype(jnp.float32))
    ).astype(jnp.bfloat16)
    tp_count = lax.axis_size("tp")
    tp_here = lax.axis_index("tp")
    expert_count = lax.axis_size("sp")
    route_rows = positions // tp_count
    top_count = routes.shape[1]
    capacity = 2 * top_count * route_rows // expert_count
    slot_total = expert_count * capacity
    projected = lax.psum_scatter(
        jnp.dot(mixer_rows, out_weight, preferred_element_type=jnp.float32).astype(jnp.bfloat16),
        "tp",
        scatter_dimension=0,
        tiled=True,
    ).astype(jnp.float32)
    own_rows = (
        lax.dynamic_slice_in_dim(residual, tp_here * route_rows, route_rows, 0).astype(jnp.float32)
        + projected
    ).astype(jnp.bfloat16)
    own_routes = lax.dynamic_slice_in_dim(routes, tp_here * route_rows, route_rows, 0)
    targets = slot_targets(own_routes, expert_count, capacity)
    outgoing = jnp.dot(
        pick_matrix(targets, slot_total),
        rms_rows(own_rows, ffn_gain),
        preferred_element_type=jnp.float32,
    ).astype(jnp.bfloat16)
    arrived = lax.all_to_all(
        outgoing.reshape(expert_count, capacity, model_width),
        "sp",
        split_axis=0,
        concat_axis=0,
        tiled=True,
    )
    partial_out = expert_apply(
        lax.all_gather(arrived.reshape(slot_total, model_width), "tp", axis=0, tiled=True),
        w_gate[0],
        w_up[0],
        w_down[0],
    )
    expert_out = lax.psum_scatter(
        partial_out.astype(jnp.bfloat16), "tp", scatter_dimension=0, tiled=True
    )
    returned = lax.all_to_all(
        expert_out.reshape(expert_count, capacity, model_width),
        "sp",
        split_axis=0,
        concat_axis=0,
        tiled=True,
    )
    picked = returned.reshape(slot_total, model_width)[targets.reshape(-1)].astype(jnp.float32)
    picked = picked.reshape(route_rows, top_count, model_width)
    own_weights = lax.dynamic_slice_in_dim(route_weights, tp_here * route_rows, route_rows, 0)
    routed = jnp.sum(picked * own_weights[:, :, None], axis=1)
    return (own_rows.astype(jnp.float32) + routed).astype(jnp.bfloat16)


MESH = pl.DeviceIdType.MESH
LANES = 128
GELU_SCALE = 0.7978845608028654


def sender(source, target, send_sem, recv_sem, peer):
    return pltpu.make_async_remote_copy(
        src_ref=source,
        dst_ref=target,
        send_sem=send_sem,
        recv_sem=recv_sem,
        device_id=peer,
        device_id_type=MESH,
    )


def greet(peers):
    barrier = pltpu.get_barrier_semaphore()
    for peer in peers:
        pl.semaphore_signal(barrier, inc=1, device_id=peer, device_id_type=MESH)
    pl.semaphore_wait(barrier, len(peers))


def one_minus_exp(value):
    series = 1.0 + value * (1.0 / 6.0)
    for order in (5.0, 4.0, 3.0, 2.0):
        series = 1.0 + value * (1.0 / order) * series
    return jnp.where(value > -0.25, -value * series, 1.0 - jnp.exp(value))


def down_by(block, distance, filler):
    count = block.shape[0]
    if distance % 8 == 0:
        top = jnp.full((distance, block.shape[1]), filler, block.dtype)
        return jnp.concatenate([top, block[: count - distance]], axis=0)
    row = lax.broadcasted_iota(jnp.int32, block.shape, 0)
    return jnp.where(row >= distance, pltpu.roll(block, distance, 0), filler)


LATE = 8


def layer_kernel(
    n_sp,
    n_tp,
    lru_hbm,
    gate_hbm,
    docs_hbm,
    taps_hbm,
    rate_hbm,
    inlet_hbm,
    decay_hbm,
    gain_hbm,
    out_w_hbm,
    residual_hbm,
    ffn_hbm,
    routes_hbm,
    shares_hbm,
    w_gate_hbm,
    w_up_hbm,
    w_down_hbm,
    out_ref,
    lru_ref,
    gate_ref,
    docs_row,
    taps_ref,
    rate_ref,
    inlet_ref,
    decay_ref,
    gain_ref,
    out_w_ref,
    ffn_ref,
    routes_ref,
    route_w_ref,
    docs_ref,
    weights_ref,
    halo_x,
    halo_d,
    carry_out,
    carry_in,
    share_in,
    run_a,
    run_b,
    parts,
    pair_in,
    z_out,
    z_in,
    squares,
    square_pair,
    square_out,
    square_in,
    res_rows,
    own_ref,
    normed_ref,
    w_gate,
    w_up,
    w_down,
    share_cols,
    blocks,
    hidden_units,
    products,
    back_in,
    joined,
    first_x,
    first_y,
    second_x,
    second_y,
    relay_a,
    relay_b,
    column,
    last_in,
    load_sem,
    res_sem,
    w_sem,
    own_sem,
    halo_s,
    halo_r,
    carry_s,
    carry_r,
    share_s,
    share_r,
    pair_s,
    pair_r,
    z_s,
    z_r,
    gz_s,
    gz_r,
    gxy_s,
    gxy_r,
    gd_s,
    gd_r,
    gp_s,
    gp_r,
    rp_s,
    rp_r,
    r1_s,
    r1_r,
    r2_s,
    r2_r,
    rz_s,
    rz_r,
):
    me_s, me_t = lax.axis_index("sp"), lax.axis_index("tp")
    n_z = n_tp // 2
    me_z, me_c = me_t // 2, me_t % 2
    rows, channels = lru_ref.shape
    width = out_w_ref.shape[1]
    piece = rows // n_tp
    pairs = (
        (lru_hbm, lru_ref),
        (docs_hbm, docs_row),
        (taps_hbm, taps_ref),
        (rate_hbm, rate_ref),
        (inlet_hbm, inlet_ref),
        (decay_hbm, decay_ref),
        (routes_hbm, routes_ref),
        (shares_hbm, route_w_ref),
        (out_w_hbm, out_w_ref),
        (gate_hbm, gate_ref),
        (gain_hbm, gain_ref),
        (ffn_hbm, ffn_ref),
    )
    loads = [
        pltpu.make_async_copy(source, target, load_sem.at[k])
        for k, (source, target) in enumerate(pairs)
    ]
    for copy in loads:
        copy.start()
    residual_copy = pltpu.make_async_copy(
        residual_hbm.at[pl.ds(pl.multiple_of(me_t * piece, piece), piece)], res_rows, res_sem
    )
    residual_copy.start()
    w_loads = [
        pltpu.make_async_copy(source, target, w_sem.at[k])
        for k, (source, target) in enumerate(
            ((w_gate_hbm, w_gate), (w_up_hbm, w_up), (w_down_hbm, w_down))
        )
    ]
    for copy in w_loads:
        copy.start()
    s_x = me_s + 1 - 2 * (me_s % 2)
    s_y = (me_s + 2) % n_sp
    s_d = n_sp - 1 - me_s
    x_peer, y_peer = (s_x, me_t), (s_y, me_t)
    partner = (me_s, me_z * 2 + 1 - me_c)
    sp_peers = [((me_s + k) % n_sp, me_t) for k in range(1, n_sp)]
    across = (me_z, me_z + 1 - 2 * (me_z % 2), n_z - 1 - me_z, (me_z + 2) % n_z)
    z_peers = [(me_s, across[k] * 2 + me_c) for k in range(1, n_z)]
    greet(sp_peers + z_peers + [partner])
    loads[0].wait()
    loads[1].wait()
    docs = jnp.transpose(jnp.broadcast_to(docs_row[...], (8, rows)))
    docs = jnp.broadcast_to(docs[:, :1], (rows, LANES))
    docs_ref[...] = docs
    halo = [
        sender(lru_ref.at[pl.ds(rows - 16, 16)], halo_x, halo_s.at[0], halo_r.at[0], sp_peers[0]),
        sender(docs_ref.at[pl.ds(rows - 8, 8)], halo_d, halo_s.at[1], halo_r.at[1], sp_peers[0]),
    ]
    for copy in halo:
        copy.start()
    loads[6].wait()
    loads[7].wait()
    expert = lax.broadcasted_iota(jnp.int32, weights_ref.shape, 0)
    shares = jnp.zeros(weights_ref.shape, jnp.float32)
    for k in range(routes_ref.shape[0]):
        shares = shares + jnp.where(
            routes_ref[k : k + 1] == expert, route_w_ref[k : k + 1], 0.0
        )
    weights_ref[...] = shares
    share = [
        sender(weights_ref, share_in.at[me_s], share_s.at[k], share_r.at[k], peer)
        for k, peer in enumerate(sp_peers)
    ]
    for copy in share:
        copy.start()
    share_in[pl.ds(me_s, 1)] = shares[None]
    for k in (2, 3, 4, 5, 9, 10, 11):
        loads[k].wait()
    for copy in halo:
        copy.wait()

    before = jnp.where(me_s == 0, jnp.int32(-1), halo_d[...])
    docs_long = jnp.concatenate([before, docs], axis=0)
    taps = taps_ref[...].astype(jnp.float32)
    starts = docs_long[7 : 7 + rows] != docs
    for group in range(channels // LANES):
        span = slice(group * LANES, (group + 1) * LANES)
        long = jnp.concatenate(
            [halo_x[:, span].astype(jnp.float32)[8:], lru_ref[:, span].astype(jnp.float32)], axis=0
        )
        total = jnp.zeros((rows, LANES), jnp.float32)
        for tap in range(taps.shape[0]):
            first = 8 - (taps.shape[0] - 1) + tap
            same = docs_long[first : first + rows] == docs
            total = total + jnp.where(same, long[first : first + rows], 0.0) * taps[tap : tap + 1, span]
        convolved = total.astype(jnp.bfloat16)
        rate = jax.nn.sigmoid(
            jnp.dot(convolved, rate_ref[group], preferred_element_type=jnp.float32)
        )
        inlet = jax.nn.sigmoid(
            jnp.dot(convolved, inlet_ref[group], preferred_element_type=jnp.float32)
        )
        minus = -decay_ref[:, span]
        soft = jnp.maximum(minus, 0.0) + jnp.log1p(jnp.exp(-jnp.abs(minus)))
        log_decay = -RATE_SCALE * rate * soft
        step = jnp.where(starts, 0.0, jnp.exp(log_decay))
        factor = jnp.where(starts, 1.0, jnp.sqrt(one_minus_exp(2.0 * log_decay)))
        state = factor * inlet * convolved.astype(jnp.float32)
        distance = 1
        while distance < rows:
            state = state + step * down_by(state, distance, 0.0)
            step = step * down_by(step, distance, 1.0)
            distance *= 2
        run_a[:, span] = step
        run_b[:, span] = state
        carry_out[:, span] = jnp.concatenate(
            [step[rows - 1 :], state[rows - 1 :], jnp.zeros((6, LANES), jnp.float32)], axis=0
        )
    carry = [
        sender(carry_out, carry_in.at[me_s], carry_s.at[k], carry_r.at[k], peer)
        for k, peer in enumerate(sp_peers)
    ]
    for copy in carry:
        copy.start()
    carry_in[pl.ds(me_s, 1)] = carry_out[...][None]
    raw = gate_ref[...].astype(jnp.float32)
    gelu = 0.5 * raw * (1.0 + jnp.tanh(GELU_SCALE * (raw + 0.044715 * raw * raw * raw)))
    gelu = gelu * gain_ref[...]
    for copy in carry:
        copy.wait()
    carried = jnp.zeros((1, channels), jnp.float32)
    for place in range(n_sp - 1):
        tile = carry_in[place]
        carried = jnp.where(place < me_s, tile[1:2] + tile[0:1] * carried, carried)
    hidden = run_b[...] + run_a[...] * carried
    row_squares = jnp.sum(hidden * hidden, axis=1, keepdims=True)
    squares[...] = jnp.broadcast_to(row_squares, (rows, LANES)).reshape(n_tp, piece, LANES)
    loads[LATE].wait()
    mixer = (hidden * gelu).astype(jnp.bfloat16)
    tile_width = min(512, width)
    for first in range(0, width, tile_width):
        span = slice(first, first + tile_width)
        product = jnp.dot(mixer, out_w_ref[:, span], preferred_element_type=jnp.float32)
        parts[:, :, span] = product.astype(jnp.bfloat16).reshape(n_tp, piece, tile_width)

    order = (across[2], across[3], across[1], me_z)
    pair = []
    for i, z in enumerate(order):
        theirs = z * 2 + 1 - me_c
        pair.append(
            (
                sender(parts.at[theirs], pair_in.at[i], pair_s.at[0, i], pair_r.at[0, i], partner),
                sender(
                    squares.at[theirs], square_pair.at[i], pair_s.at[1, i], pair_r.at[1, i], partner
                ),
            )
        )
        for copy in pair[-1]:
            copy.start()
    z_copies = []
    for i, z in enumerate(order):
        mine = z * 2 + me_c
        for copy in pair[i]:
            copy.wait_recv()
        z_out[i] = (
            parts[mine].astype(jnp.float32) + pair_in[i].astype(jnp.float32)
        ).astype(jnp.bfloat16)
        square_out[i] = squares[mine] + square_pair[i]
        if i < n_z - 1:
            peer = (me_s, mine)
            copies = (
                sender(z_out.at[i], z_in.at[i], z_s.at[0, i], z_r.at[0, i], peer),
                sender(square_out.at[i], square_in.at[i], z_s.at[1, i], z_r.at[1, i], peer),
            )
            for copy in copies:
                copy.start()
            z_copies.append(copies)
    summed = z_out[n_z - 1].astype(jnp.float32)
    square_sum = square_out[n_z - 1]
    for i in range(n_z - 1):
        for copy in z_copies[i]:
            copy.wait_recv()
        summed = summed + z_in[i].astype(jnp.float32)
        square_sum = square_sum + square_in[i]
    inverse = lax.rsqrt(square_sum[:, :1] / (channels * n_tp) + EPSILON)
    residual_copy.wait()
    own = (res_rows[...].astype(jnp.float32) + summed * inverse).astype(jnp.bfloat16)
    own_ref[...] = own
    floated = own.astype(jnp.float32)
    inverse = lax.rsqrt(jnp.mean(floated * floated, axis=1, keepdims=True) + EPSILON)
    normed_ref[...] = (floated * inverse * ffn_ref[...]).astype(jnp.bfloat16)

    half = width // 2
    lower, upper = pl.ds(0, half), pl.ds(half, half)
    sent = []

    def push(source, target, sems, slot, peer):
        copy = sender(source, target, sems[0].at[slot], sems[1].at[slot], peer)
        copy.start()
        sent.append(copy)
        return copy

    gz, gxy, gd, gp = (gz_s, gz_r), (gxy_s, gxy_r), (gd_s, gd_r), (gp_s, gp_r)
    rp, r1, r2, rz = (rp_s, rp_r), (r1_s, r1_r), (r2_s, r2_r), (rz_s, rz_r)
    from_z, from_x, from_y, from_da, from_db, from_pair = {}, {}, {}, {}, {}, {}

    def spread(i):
        block = blocks.at[i, me_s, me_c]
        if i == 0:
            source = normed_ref
        else:
            from_z[i].wait_recv()
            source = block
        from_x[i] = push(source, block, gxy, (0, i), x_peer)
        from_y[i] = push(source, block, gxy, (1, i), y_peer)
        from_pair[0, i] = push(source, block, gp, (0, i), partner)

    def relay(i):
        from_x[i].wait_recv()
        block, part = blocks.at[i, s_x, me_c], blocks.at[i, s_x, me_c, :, lower]
        from_da[i] = push(part, part, gd, (0, i), y_peer)
        from_pair[1, i] = push(block, block, gp, (1, i), partner)
        from_y[i].wait_recv()
        block, part = blocks.at[i, s_y, me_c], blocks.at[i, s_y, me_c, :, upper]
        from_db[i] = push(part, part, gd, (1, i), x_peer)
        from_pair[2, i] = push(block, block, gp, (2, i), partner)

    def hand_over(i):
        from_da[i].wait_recv()
        part = blocks.at[i, s_d, me_c, :, lower]
        from_pair[3, i] = push(part, part, gp, (3, i), partner)
        from_db[i].wait_recv()
        part = blocks.at[i, s_d, me_c, :, upper]
        from_pair[4, i] = push(part, part, gp, (4, i), partner)

    own_copy = pltpu.make_async_copy(normed_ref, blocks.at[0, me_s, me_c], own_sem)
    own_copy.start()
    spread(0)
    for k in range(n_z - 1):
        from_z[k + 1] = push(normed_ref, blocks.at[k + 1, me_s, me_c], gz, k, z_peers[k])
    for copy in share:
        copy.wait()
    for place in range(n_sp):
        turned = jnp.transpose(share_in[place])
        lane = lax.broadcasted_iota(jnp.int32, turned.shape, 1)
        chosen = jnp.sum(jnp.where(lane == me_s, turned, 0.0), axis=1, keepdims=True)
        share_cols[place] = jnp.broadcast_to(chosen, (rows, LANES))

    ff = w_gate.shape[1]
    f_tile, d_tile = 256, min(512, width)
    count = n_sp * 2 * piece
    back, first_xs, first_ys, second_xs, second_ys, back_z = {}, {}, {}, {}, {}, {}

    def rise(i):
        for k in range(5):
            from_pair[k, i].wait_recv()
        tokens = blocks[i].reshape(count, width)

        def up_step(step, _):
            span = pl.ds(pl.multiple_of(step * f_tile, f_tile), f_tile)
            gate_part = jnp.dot(tokens, w_gate[:, span], preferred_element_type=jnp.float32)
            up_part = jnp.dot(tokens, w_up[:, span], preferred_element_type=jnp.float32)
            hidden_units[:, span] = (gate_part * jax.nn.sigmoid(gate_part) * up_part).astype(
                jnp.bfloat16
            )
            return 0

        lax.fori_loop(0, ff // f_tile, up_step, 0)

    def fall(i):
        z = across[i]
        first = pl.multiple_of(z * (2 * piece), 2 * piece)
        scale = share_cols[:, pl.ds(first, 2 * piece), :].reshape(count, LANES)[:, :1]
        units = hidden_units[...]

        def down_step(step, _):
            span = pl.ds(pl.multiple_of(step * d_tile, d_tile), d_tile)
            product = jnp.dot(units, w_down[:, span], preferred_element_type=jnp.float32) * scale
            products[i, :, :, :, span] = product.astype(jnp.bfloat16).reshape(
                n_sp, 2, piece, d_tile
            )
            return 0

        lax.fori_loop(0, width // d_tile, down_step, 0)
        for k, group in enumerate((s_d, s_x, s_y, me_s)):
            back[k, i] = push(
                products.at[i, group, 1 - me_c], back_in.at[i, k], rp, (k, i), partner
            )

    def join(i):
        for k, group in enumerate((s_d, s_x, s_y, me_s)):
            back[k, i].wait_recv()
            joined[i, k] = (
                products[i, group, me_c].astype(jnp.float32) + back_in[i, k].astype(jnp.float32)
            ).astype(jnp.bfloat16)
            if k == 0:
                first_xs[1, i] = push(
                    joined.at[i, 0, :, lower], first_x.at[1, i], r1, (2, i), x_peer
                )
                first_ys[1, i] = push(
                    joined.at[i, 0, :, upper], first_y.at[1, i], r1, (3, i), y_peer
                )
            elif k == 1:
                first_xs[0, i] = push(
                    joined.at[i, 1, :, lower], first_x.at[0, i], r1, (0, i), x_peer
                )
            elif k == 2:
                first_ys[0, i] = push(
                    joined.at[i, 2, :, upper], first_y.at[0, i], r1, (1, i), y_peer
                )

    def turn(i):
        first_xs[1, i].wait_recv()
        relay_a[i] = (
            joined[i, 2, :, :half].astype(jnp.float32) + first_x[1, i].astype(jnp.float32)
        ).astype(jnp.bfloat16)
        second_ys[i] = push(relay_a.at[i], second_y.at[i], r2, (0, i), y_peer)
        first_ys[1, i].wait_recv()
        relay_b[i] = (
            joined[i, 1, :, half:].astype(jnp.float32) + first_y[1, i].astype(jnp.float32)
        ).astype(jnp.bfloat16)
        second_xs[i] = push(relay_b.at[i], second_x.at[i], r2, (1, i), x_peer)

    def finish(i):
        for copies in (first_xs, first_ys):
            copies[0, i].wait_recv()
        for copies in (second_xs, second_ys):
            copies[i].wait_recv()
        low = (
            joined[i, 3, :, :half].astype(jnp.float32)
            + first_x[0, i].astype(jnp.float32)
            + second_y[i].astype(jnp.float32)
        )
        high = (
            joined[i, 3, :, half:].astype(jnp.float32)
            + first_y[0, i].astype(jnp.float32)
            + second_x[i].astype(jnp.float32)
        )
        column[i] = jnp.concatenate([low, high], axis=1).astype(jnp.bfloat16)
        if i > 0:
            peer = z_peers[i - 1]
            back_z[i] = push(column.at[i], last_in.at[i], rz, i, peer)

    own_copy.wait()
    for copy in w_loads:
        copy.wait()
    last = n_z - 1
    spread(1)
    for tick in range(-2, n_z + 2):
        plan = (
            (relay, tick + 2),
            (spread, tick + 3),
            (hand_over, tick + 1),
            (rise, tick),
            (join, tick - 1),
            (finish, tick - 2),
            (fall, tick),
            (turn, tick - 1),
        )
        for stage, i in plan:
            if 0 <= i <= last and not (stage is spread and i <= 1):
                stage(i)
    total = own_ref[...].astype(jnp.float32) + column[0].astype(jnp.float32)
    for i in range(1, n_z):
        back_z[i].wait_recv()
        total = total + last_in[i].astype(jnp.float32)
    out_ref[...] = total.astype(jnp.bfloat16)
    for copies in pair + z_copies:
        for copy in copies:
            copy.wait_send()
    for copy in sent:
        copy.wait_send()


def dense_local(
    lru_input,
    gate_input,
    documents,
    conv_taps,
    rate_weight,
    inlet_weight,
    decay_param,
    lru_gain,
    out_weight,
    residual,
    ffn_gain,
    routes,
    route_weights,
    w_gate,
    w_up,
    w_down,
):
    n_sp, n_tp = lax.axis_size("sp"), lax.axis_size("tp")
    n_z = n_tp // 2
    rows, channels = lru_input.shape
    width = residual.shape[1]
    ff = w_gate.shape[2]
    piece = rows // n_tp
    padded = -(-n_sp // 8) * 8
    vmem = pl.BlockSpec(memory_space=pltpu.VMEM)
    half = width // 2
    top = routes.shape[1]
    hbm = pl.BlockSpec(memory_space=pl.ANY)
    bf16, f32 = jnp.bfloat16, jnp.float32
    dma = pltpu.SemaphoreType.DMA
    rows_buffer = pltpu.VMEM((n_z, piece, width), bf16)
    half_buffer = pltpu.VMEM((n_z, piece, half), bf16)
    chunks = pltpu.VMEM((n_z, n_sp, 2, piece, width), bf16)
    groups = pltpu.VMEM((n_z, n_sp, piece, width), bf16)
    square_buffer = pltpu.VMEM((n_z, piece, LANES), f32)
    shapes = (
        [(2,)] * 2
        + [(n_sp,)] * 4
        + [(2, n_z)] * 4
        + [(n_z,)] * 2
        + [(2, n_z)] * 4
        + [(5, n_z)] * 2
        + [(4, n_z)] * 4
        + [(2, n_z)] * 2
        + [(n_z,)] * 2
    )
    return pl.pallas_call(
        functools.partial(layer_kernel, n_sp, n_tp),
        out_shape=jax.ShapeDtypeStruct((piece, width), bf16),
        in_specs=[hbm] * 16,
        out_specs=vmem,
        scratch_shapes=[
            pltpu.VMEM((rows, channels), bf16),
            pltpu.VMEM((rows, channels), bf16),
            pltpu.VMEM((1, rows), jnp.int32),
            pltpu.VMEM(conv_taps.shape, bf16),
            pltpu.VMEM(rate_weight.shape, bf16),
            pltpu.VMEM(inlet_weight.shape, bf16),
            pltpu.VMEM((1, channels), f32),
            pltpu.VMEM((1, channels), f32),
            pltpu.VMEM((channels, width), bf16),
            pltpu.VMEM((1, width), f32),
            pltpu.VMEM((top, rows), jnp.int32),
            pltpu.VMEM((top, rows), f32),
            pltpu.VMEM((rows, LANES), jnp.int32),
            pltpu.VMEM((padded, rows), f32),
            pltpu.VMEM((16, channels), bf16),
            pltpu.VMEM((8, LANES), jnp.int32),
            pltpu.VMEM((8, channels), f32),
            pltpu.VMEM((n_sp, 8, channels), f32),
            pltpu.VMEM((n_sp, padded, rows), f32),
            pltpu.VMEM((rows, channels), f32),
            pltpu.VMEM((rows, channels), f32),
            pltpu.VMEM((n_tp, piece, width), bf16),
            rows_buffer,
            rows_buffer,
            rows_buffer,
            pltpu.VMEM((n_tp, piece, LANES), f32),
            square_buffer,
            square_buffer,
            square_buffer,
            pltpu.VMEM((piece, width), bf16),
            pltpu.VMEM((piece, width), bf16),
            pltpu.VMEM((piece, width), bf16),
            pltpu.VMEM((width, ff), bf16),
            pltpu.VMEM((width, ff), bf16),
            pltpu.VMEM((ff, width), bf16),
            pltpu.VMEM((n_sp, rows, LANES), f32),
            chunks,
            pltpu.VMEM((n_sp * 2 * piece, ff), bf16),
            chunks,
            groups,
            groups,
            pltpu.VMEM((2, n_z, piece, half), bf16),
            pltpu.VMEM((2, n_z, piece, half), bf16),
            half_buffer,
            half_buffer,
            half_buffer,
            half_buffer,
            rows_buffer,
            rows_buffer,
            dma((12,)),
            dma,
            dma((3,)),
            dma,
        ]
        + [dma(shape) for shape in shapes],
        compiler_params=pltpu.CompilerParams(
            collective_id=0, has_side_effects=True, vmem_limit_bytes=60 * 2**20
        ),
    )(
        lru_input,
        gate_input,
        documents[None, :],
        conv_taps,
        rate_weight,
        inlet_weight,
        decay_param[None, :],
        lru_gain[None, :],
        out_weight,
        residual,
        ffn_gain[None, :],
        routes.T,
        route_weights.T,
        w_gate[0],
        w_up[0],
        w_down[0],
    )


def solution(mesh):
    n_sp, n_tp = mesh.shape["sp"], mesh.shape["tp"]
    body = dense_local if n_sp == 4 and n_tp == 8 else local
    return jax.shard_map(
        body,
        mesh=mesh,
        in_specs=(
            P("sp", "tp"),
            P("sp", "tp"),
            P("sp"),
            P(None, "tp"),
            P("tp", None, None),
            P("tp", None, None),
            P("tp"),
            P("tp"),
            P("tp", None),
            P("sp", None),
            P(),
            P("sp", None),
            P("sp", None),
            P("sp", None, "tp"),
            P("sp", None, "tp"),
            P("sp", "tp", None),
        ),
        out_specs=P(("sp", "tp"), None),
        check_vma=False,
    )
```
